32 devices in a mesh: sp: 8 (over z, x), dp: 4 (over y, core).
Axes of the slice: x: 2, y: 2, z: 4, core: 2. Of those that a mesh axis runs over, the one named last changes fastest.
Arguments:
- queries: bfloat16 [4, 1024, 2048], P('dp', 'sp'), may hold values from -12 to 12
- key_rows: bfloat16 [4, 1024, 2048], P('dp', 'sp'), may hold values from -12 to 12
- value_rows: bfloat16 [4, 1024, 2048], P('dp', 'sp'), may hold values from -6 to 6
- lambdas: float32 [16], P('sp'), may hold values from 0.3 to 0.8
- head_gain: float32 [128], replicated, may hold values from 0.1 to 1.9
- out_weight: bfloat16 [2048, 2048], replicated, may hold values from -0.125 to 0.125
- residual: bfloat16 [4, 1024, 2048], P('dp', 'sp'), may hold values from -6 to 6
- mixer_gain: float32 [2048], replicated, may hold values from 0.1 to 1.9
- channel_gain: float32 [2048], replicated, may hold values from 0.1 to 1.9
- expert_gain: float32 [2048], replicated, may hold values from 0.1 to 1.9
- routes: int32 [4, 1024, 2], P('dp', 'sp'), may hold values from 0 to 7, all different within a row; in each aligned block of 128 rows (0 to 127, 128 to 255, ..., all dimensions but the last counted through in order) at most 48 rows name the same one
- route_logits: float32 [4, 1024, 2], P('dp', 'sp'), may hold values from -5 to 5
- gate_weight: bfloat16 [8, 2048, 4096], P('sp', None, 'dp'), may hold values from -0.125 to 0.125
- up_weight: bfloat16 [8, 2048, 4096], P('sp', None, 'dp'), may hold values from -0.125 to 0.125
- down_weight: bfloat16 [8, 4096, 2048], P('sp', 'dp'), may hold values from -0.09375 to 0.09375
Outputs:
- updated: bfloat16 [4, 1024, 2048], P('dp', 'sp')
The draws below stay inside these ranges and needn't reach their ends.
Inputs may be any that keep to these rules, and one draw needn't show every extreme that they name: `routes`: among the rows of one device no expert is named by more than 48 rows; in some of these blocks one expert is named by exactly 48.
All inputs are finite; a program needn't handle non-finite values.
Results may differ from the reference program's by a relative error of at most 0.014.
Values may be sent and summed in bfloat16 or wider, within the bound.
A program may use at most 128 MiB of HBM per device.

```python
import math
import jax
import jax.numpy as jnp
import numpy as np
from jax import lax

D = 2048
HEADS = 16
HD = 64
FF = 4096
TOP = 2
TOK_DEV = 128
LEN = 1024
SEQS = 4
EXPERTS = 8
CAP = 48
N_SP = 8
N_DP = 4


def draw_queries(key, part):
    base = jnp.clip(1.32 * jax.random.normal(jax.random.fold_in(key, 1), (SEQS, LEN, HEADS * 2 * HD), jnp.float32), -12.0, 12.0)
    return base.astype(jnp.bfloat16)


def draw_key_rows(key, part):
    base = jnp.clip(1.32 * jax.random.normal(jax.random.fold_in(key, 2), (SEQS, LEN, HEADS * 2 * HD), jnp.float32), -12.0, 12.0)
    return base.astype(jnp.bfloat16)


def block_scale(stream_key, shape, cuts, low, top_value):
    factor_of, own = 1.0, jax.random.fold_in(stream_key, 6)
    for position, parts in cuts:
        steps = jnp.exp(jax.random.uniform(jax.random.fold_in(own, position), (parts,), jnp.float32, low / len(cuts), top_value / len(cuts)))
        factor_of = factor_of * jnp.repeat(steps, shape[position] // parts).reshape([-1 if axis == position else 1 for axis in range(len(shape))])
    return factor_of


def routed_block(rng, own, number, rows, count, top, most, skew):
    ranking = jax.random.permutation(rng, count)
    heavy_load, usual = load_shares(count, rows * top, most, skew, True), load_shares(count, rows * top, most, skew, False)
    places = jnp.arange(count)

    def named(sizes, turn):
        used = int((sizes > 0).sum())
        fixed = max(1, used // 4)
        passed = fixed + (places - fixed + turn * (used - fixed)) % max(1, count - fixed)
        return jnp.zeros((count,), jnp.int32).at[ranking[jnp.where(places < fixed, places, passed)]].set(jnp.asarray(sizes, jnp.int32))

    sizes = jnp.where(number % 4 == 0, named(heavy_load, number // 4), named(usual, number - number // 4 - 1))
    mixed = jax.random.permutation(jax.random.fold_in(own, 3), count)
    giver, receiver = mixed[0:count // 2 * 2:2], mixed[1:count // 2 * 2:2]
    slack = jnp.minimum(sizes[giver] - 1, most - sizes[receiver]) // 2
    slack = jnp.where((giver == ranking[0]) | (receiver == ranking[0]) | (sizes[receiver] == 0), 0, jnp.maximum(slack, 0))
    passed = jax.random.randint(jax.random.fold_in(own, 4), (count // 2,), 0, 1 << 20) % (slack + 1)
    sizes = sizes.at[giver].add(-passed).at[receiver].add(passed)
    labels = jnp.searchsorted(jnp.cumsum(sizes), jnp.arange(rows * top), side="right").astype(jnp.int32)
    table = labels.reshape(top, rows).T
    table = table[jax.random.permutation(jax.random.fold_in(own, 1), rows)]
    turn = jax.random.randint(jax.random.fold_in(own, 2), (rows, 1), 0, top)
    return jnp.take_along_axis(table, (jnp.arange(top)[None, :] + turn) % top, axis=1)


def load_shares(number_of, total, most, lean, full):
    loads = [(1 << 20) // math.isqrt(grade ** lean) + 1 for grade in range(1, number_of + 1)]
    largest = most if full else min(most, max(-(-total // number_of), total * loads[0] // sum(loads)))
    least = 1 if total - largest >= number_of - 1 else 0
    holding, rest = [largest] + [least] * (number_of - 1), total - largest - least * (number_of - 1)
    while rest > 0:
        free = [i for i in range(1, number_of) if holding[i] < largest] or [i for i in range(1, number_of) if holding[i] < most]
        mass, left = sum([loads[i] for i in free]), rest
        for i in free:
            more = min(most - holding[i], max(1, left * loads[i] // mass), rest)
            holding[i] = holding[i] + more
            rest = rest - more
    return np.array(holding)


def scatter_about(key, shape, deviation, reach, pieces=(), kind=jnp.bfloat16):
    values = deviation * jax.random.normal(key, shape, jnp.float32)
    if pieces:
        values = values * block_scale(key, shape, pieces, -0.22, 0.18)
    return jnp.clip(values, -reach, reach).astype(kind)


def setup_inputs(seed: int = 0) -> dict:
    seeds = jax.random.split(jax.random.key(seed), 16)
    queries = draw_queries(jax.random.fold_in(seeds[15], 71), 0)
    key_rows = draw_key_rows(jax.random.fold_in(seeds[15], 71), 0)
    value_rows = scatter_about(seeds[2], (SEQS, LEN, HEADS * 2 * HD), 1.0, 6.0, ((0, 4), (1, 8)))
    lambdas = jnp.clip(0.3 + 0.5 * jax.random.uniform(seeds[3], (HEADS,), jnp.float32) ** block_scale(seeds[3], (HEADS,), ((0, 8),), -0.2, 0.2), 0.3, 0.8)
    head_gain = jnp.clip(1.0 + 0.18 * jax.random.normal(seeds[4], (2 * HD,), jnp.float32), 0.1, 1.9)
    out_weight = scatter_about(seeds[5], (HEADS * 2 * HD, D), (HEADS * 2 * HD) ** -0.5, 0.125)
    residual = scatter_about(seeds[6], (SEQS, LEN, D), 1.0, 6.0, ((0, 4), (1, 8)))
    mixer_gain = jnp.clip(1.0 + 0.18 * jax.random.normal(seeds[7], (D,), jnp.float32), 0.1, 1.9)
    channel_gain = jnp.clip(1.0 + 0.18 * jax.random.normal(seeds[8], (D,), jnp.float32), 0.1, 1.9)
    expert_gain = jnp.clip(1.0 + 0.18 * jax.random.normal(seeds[9], (D,), jnp.float32), 0.1, 1.9)
    routes_keys = jax.random.split(jax.random.fold_in(seeds[10], 1), SEQS * LEN // TOK_DEV)
    routes_turns = jax.random.permutation(jax.random.fold_in(seeds[10], 3), SEQS * LEN // TOK_DEV)
    routes = jax.vmap(lambda own, number: routed_block(jax.random.fold_in(seeds[10], 2), own, number, TOK_DEV, EXPERTS, TOP, CAP, 2))(routes_keys, routes_turns).reshape((SEQS, LEN, TOP))
    route_logits = scatter_about(seeds[11], (SEQS, LEN, TOP), 1.0, 5.0, ((0, 4), (1, 8)), jnp.float32)
    gate_weight = scatter_about(seeds[12], (EXPERTS, D, FF), D ** -0.5, 0.125, ((0, 8), (2, 4)))
    up_weight = scatter_about(seeds[13], (EXPERTS, D, FF), D ** -0.5, 0.125, ((0, 8), (2, 4)))
    down_weight = scatter_about(seeds[14], (EXPERTS, FF, D), FF ** -0.5, 0.09375, ((0, 8), (1, 4)))
    return {"queries": queries, "key_rows": key_rows, "value_rows": value_rows, "lambdas": lambdas, "head_gain": head_gain, "out_weight": out_weight, "residual": residual, "mixer_gain": mixer_gain, "channel_gain": channel_gain, "expert_gain": expert_gain, "routes": routes, "route_logits": route_logits, "gate_weight": gate_weight, "up_weight": up_weight, "down_weight": down_weight}


def rotate(field):
    dim_full = field.shape[-1]
    dim_half = dim_full // 2
    inverse = 1.0 / 10000.0 ** (jnp.arange(0, dim_full, 2, dtype=jnp.float32) / dim_full)
    angles = jnp.arange(field.shape[-4], dtype=jnp.float32)[:, None] * inverse[None, :]
    cosine = jnp.cos(angles)[:, None, None, :]
    sine_table = jnp.sin(angles)[:, None, None, :]
    floats = field.astype(jnp.float32)
    front_part = floats[..., :dim_half]
    second = floats[..., dim_half:]
    turned = jnp.concatenate([front_part * cosine - second * sine_table, second * cosine + front_part * sine_table], axis=-1)
    return turned.astype(jnp.bfloat16)

def rms_scale(values, epsilon):
    return values * lax.rsqrt(lax.optimization_barrier(jnp.mean(values * values, axis=-1, keepdims=True)) + epsilon)

def reference(queries, key_rows, value_rows, lambdas, head_gain, out_weight, residual, mixer_gain, channel_gain, expert_gain, routes, route_logits, gate_weight, up_weight, down_weight):
    seq_count = queries.shape[0]
    length = queries.shape[1]
    query_rot = rotate(queries.reshape(seq_count, length, HEADS, 2, HD))
    keys_rot = rotate(key_rows.reshape(seq_count, length, HEADS, 2, HD))
    query_items = query_rot.transpose(0, 2, 1, 3, 4).reshape(seq_count * HEADS, length, 2, HD)
    key_items = keys_rot.transpose(0, 2, 1, 3, 4).reshape(seq_count * HEADS, length, 2, HD)
    value_items = value_rows.reshape(seq_count, length, HEADS, 2 * HD).transpose(0, 2, 1, 3).reshape(seq_count * HEADS, length, 2 * HD)
    lambda_items = jnp.tile(lambdas, seq_count)

    def one_head(item):
        query_one, key_one, value_one, lambda_one = item
        scores = jnp.einsum('qcd,kcd->cqk', query_one.astype(jnp.float32), key_one.astype(jnp.float32)) * HD ** (-0.5)
        probs = jax.nn.softmax(scores, axis=-1)
        mixing = (probs[0] - lambda_one * probs[1]).astype(jnp.bfloat16)
        head_mix = jnp.dot(mixing, value_one, preferred_element_type=jnp.float32)
        return (rms_scale(head_mix, 1e-05) * head_gain).astype(jnp.bfloat16)
    heads_out = lax.map(one_head, (query_items, key_items, value_items, lambda_items))
    attended = heads_out.reshape(seq_count, HEADS, length, 2 * HD).transpose(0, 2, 1, 3).reshape(seq_count * length, HEADS * 2 * HD)
    projected = jnp.dot(attended, out_weight, preferred_element_type=jnp.float32)
    stream = (residual.reshape(seq_count * length, D).astype(jnp.float32) + rms_scale(projected, 1e-06) * mixer_gain).astype(jnp.bfloat16)
    normed = (rms_scale(stream.astype(jnp.float32), 1e-06) * channel_gain).astype(jnp.bfloat16)
    choice_ids = routes.reshape(-1).astype(jnp.int32)
    token_of = jnp.arange(choice_ids.shape[0], dtype=jnp.int32) // TOP
    shares = jax.nn.softmax(route_logits.reshape(-1, TOP), axis=-1).reshape(-1)
    limit = N_SP * N_DP * CAP
    block_units = FF // N_DP

    def per_expert(total, expert):
        others = (choice_ids != expert).astype(jnp.int32)
        order = jnp.argsort(others, stable=True)[:limit].astype(jnp.int32)
        count = jnp.sum(1 - others)
        valid = (jnp.arange(limit, dtype=jnp.int32) < count).astype(jnp.float32)
        tok_index = token_of[order]
        rows = normed[tok_index]
        gate_act = jnp.dot(rows, gate_weight[expert], preferred_element_type=jnp.float32)
        up_act = jnp.dot(rows, up_weight[expert], preferred_element_type=jnp.float32)
        hidden = (jax.nn.silu(gate_act) * up_act).astype(jnp.bfloat16)
        expert_sum = jnp.zeros((limit, D), jnp.float32)
        for block in range(N_DP):
            part = jnp.dot(hidden[:, block * block_units:(block + 1) * block_units], down_weight[expert, block * block_units:(block + 1) * block_units], preferred_element_type=jnp.float32)
            expert_sum = expert_sum + lax.optimization_barrier(part.astype(jnp.bfloat16)).astype(jnp.float32)
        expert_out = expert_sum.astype(jnp.bfloat16).astype(jnp.float32)
        weighted = expert_out * (shares[order] * valid)[:, None]
        return (total.at[tok_index].add(weighted), None)
    combined, _ = lax.scan(per_expert, jnp.zeros((seq_count * length, D), jnp.float32), jnp.arange(EXPERTS, dtype=jnp.int32))
    updated = stream.astype(jnp.float32) + rms_scale(combined, 1e-06) * expert_gain
    return updated.astype(jnp.bfloat16).reshape(seq_count, length, D)
```

```python
import functools
import math

import jax
import jax.numpy as jnp
import numpy as np
from jax import lax
from jax.experimental import pallas as pl
from jax.experimental.pallas import tpu as pltpu
from jax.sharding import PartitionSpec as P


MESH = pl.DeviceIdType.MESH
WIDTH = 2


def layer_kernel(
    count,
    groups,
    query_hbm,
    key_hbm,
    value_hbm,
    cos_hbm,
    sin_hbm,
    lambda_ref,
    head_gain_ref,
    residual_hbm,
    mixer_gain_ref,
    channel_gain_ref,
    expert_gain_ref,
    routes_ref,
    logits_ref,
    weight_hbm,
    gate_hbm,
    up_hbm,
    down_hbm,
    out_hbm,
    query_ref,
    key_ref,
    value_ref,
    cos_ref,
    sin_ref,
    residual_ref,
    query_out,
    key_out,
    query_in,
    key_in,
    value_in,
    head_out,
    token_rows,
    projected,
    square_ref,
    stream_ref,
    normed_ref,
    place_ref,
    high_ref,
    low_ref,
    pool,
    outgoing,
    arrived,
    own,
    cross_in,
    returned,
    hidden,
    gate_w,
    up_w,
    down_w,
    in_sem,
    weight_sem,
    expert_sem,
    out_sem,
    in_send,
    in_recv,
    head_send,
    head_recv,
    a_send,
    a_recv,
    b_send,
    b_recv,
    c_send,
    c_recv,
    d_send,
    d_recv,
    e_send,
    e_recv,
    f_send,
    f_recv,
):
    me = lax.axis_index("sp")
    dp = lax.axis_index("dp")
    chip, core = dp // 2, dp % 2
    tokens, model = query_ref.shape
    lanes = head_gain_ref.shape[1]
    heads = lambda_ref.shape[0]
    map_dim = lanes // 2
    scale = map_dim ** (-0.5)
    capacity = outgoing.shape[1]
    units = gate_w.shape[1]
    wide = math.gcd(model, 512)
    half = jnp.bfloat16

    def peer(k):
        total, bit = 0, 1
        while bit < count:
            a, b = (me // bit) % 2, (k // bit) % 2
            total = total + bit * (a + b - 2 * a * b)
            bit *= 2
        return total

    other = {"sp": me, "dp": chip * 2 + (1 - core)}

    def chip_at(step):
        return {"sp": me, "dp": ((chip + step + groups) % groups) * 2 + core}

    def sp_at(k):
        return {"sp": peer(k), "dp": dp}

    def columns(owner, h):
        return pl.ds(pl.multiple_of((owner * heads + h) * lanes, lanes), lanes)

    def tile_of(n, size):
        return pl.ds(pl.multiple_of(n * size, size), size)

    def remote(src, dst, send, recv, device):
        return pltpu.make_async_remote_copy(
            src_ref=src, dst_ref=dst, send_sem=send, recv_sem=recv, device_id=device, device_id_type=MESH
        )

    rows_here = pl.ds(pl.multiple_of(me * tokens, tokens), tokens)
    inputs = [
        pltpu.make_async_copy(src, dst, in_sem.at[i])
        for i, (src, dst) in enumerate(
            (
                (value_hbm, value_ref),
                (key_hbm, key_ref),
                (cos_hbm.at[rows_here], cos_ref),
                (sin_hbm.at[rows_here], sin_ref),
                (query_hbm, query_ref),
                (residual_hbm, residual_ref),
            )
        )
    ]
    for copy in inputs:
        copy.start()

    def weight_load(h, o):
        return pltpu.make_async_copy(
            weight_hbm.at[columns(o, h)],
            pool.at[pl.ds(pl.multiple_of((h * count + o) * lanes, lanes), lanes)],
            weight_sem.at[h, o],
        )

    expert_loads = [
        pltpu.make_async_copy(src, dst, expert_sem.at[i])
        for i, (src, dst) in enumerate(((gate_hbm, gate_w), (up_hbm, up_w), (down_hbm, down_w)))
    ]

    barrier = pltpu.get_barrier_semaphore()
    peers = [sp_at(k) for k in range(1, count)] + [chip_at(j) for j in range(1, groups)] + [other]
    for device in peers:
        pl.semaphore_signal(barrier, inc=1, device_id=device, device_id_type=MESH)

    def inward(h, k, i):
        sources = (value_ref.at[:, columns(peer(k), h)], query_out.at[h, k], key_out.at[h, k])
        targets = (value_in.at[h, k], query_in.at[h, k], key_in.at[h, k])
        return remote(sources[i], targets[i], in_send.at[h, i, k], in_recv.at[h, i, k], sp_at(k))

    def outward(h, k):
        return remote(
            head_out.at[h, k],
            token_rows.at[h, :, tile_of(me, lanes)],
            head_send.at[h, k],
            head_recv.at[h, k],
            sp_at(k),
        )

    first_half = lax.broadcasted_iota(jnp.int32, (tokens, lanes), 1) % map_dim < map_dim // 2

    def turned(ref, cols):
        x = ref[:, cols].astype(jnp.float32)
        ahead = pltpu.roll(x, lanes - map_dim // 2, 1)
        behind = pltpu.roll(x, map_dim // 2, 1)
        return x * cos_ref[...] + jnp.where(first_half, ahead, behind) * sin_ref[...]

    def turned_query(cols):
        return (turned(query_ref, cols) * scale).astype(half)

    def turned_key(cols):
        return turned(key_ref, cols).astype(half)

    inputs[0].wait()
    pl.semaphore_wait(barrier, len(peers))

    for h in range(heads):

        @pl.loop(1, count)
        def _(k):
            inward(h, k, 0).start()

        if h == 0:
            for copy in inputs[1:4]:
                copy.wait()

        @pl.loop(1, count)
        def _(k):
            key_out[h, k] = turned_key(columns(peer(k), h))

        @pl.loop(1, count)
        def _(k):
            inward(h, k, 2).start()

        if h == 0:
            inputs[4].wait()

        @pl.loop(1, count)
        def _(k):
            query_out[h, k] = turned_query(columns(peer(k), h))

        @pl.loop(1, count)
        def _(k):
            inward(h, count - k, 1).start()

    for h in range(heads):
        query_in[h, 0] = turned_query(columns(me, h))
        key_in[h, 0] = turned_key(columns(me, h))
        value_in[h, 0] = value_ref[:, columns(me, h)]

    for h in range(heads):

        @pl.loop(0, count)
        def _(o):
            weight_load(h, o).start()

    for copy in expert_loads:
        copy.start()

    top = routes_ref.shape[0]
    slots = count * capacity
    ranks = max(16, count)
    experts = lax.broadcasted_iota(jnp.int32, (ranks, tokens), 0)
    places = lax.broadcasted_iota(jnp.int32, (slots, tokens), 0)
    upper = lax.broadcasted_iota(jnp.int32, (tokens, tokens), 0)
    upper = (upper <= lax.broadcasted_iota(jnp.int32, (tokens, tokens), 1)).astype(half)
    logits = logits_ref[...]
    odds = jnp.exp(logits - jnp.max(logits, axis=0, keepdims=True))
    shares = odds / jnp.sum(odds, axis=0, keepdims=True)
    used = jnp.zeros((ranks, 1), jnp.float32)
    mix = jnp.zeros((slots, tokens), jnp.float32)
    place = jnp.zeros((slots, tokens), jnp.float32)
    for i in range(top):
        ranked = jnp.bitwise_xor(routes_ref[i : i + 1, :], me)
        named = (experts == ranked).astype(jnp.float32)
        running = jnp.dot(named.astype(half), upper, preferred_element_type=jnp.float32)
        slot = jnp.sum(named * (running + used), axis=0, keepdims=True).astype(jnp.int32) - 1
        used = used + jnp.sum(named, axis=1, keepdims=True)
        hit = places == ranked * capacity + slot
        mix = mix + jnp.where(hit, shares[i : i + 1, :], 0.0)
        place = place + jnp.where(hit, 1.0, 0.0)
    place_ref[...] = place.astype(half)
    mix = mix.T
    high = mix.astype(half)
    high_ref[...] = high
    low_ref[...] = (mix - high.astype(jnp.float32)).astype(half)

    rows = WIDTH * tokens
    length = count * tokens
    in_first = lax.broadcasted_iota(jnp.int32, (rows, lanes), 1) < map_dim

    def part_of(total):
        return jnp.exp(total - jnp.max(total, axis=-1, keepdims=True))

    for h in range(heads):

        @pl.loop(1, count)
        def _(k):
            inward(h, k, 0).wait_recv()
            inward(h, k, 2).wait_recv()

        @pl.loop(0, count // WIDTH)
        def _(step):
            b = count // WIDTH - 1 - step
            for i in range(WIDTH):
                k = b * WIDTH + i

                @pl.when(k > 0)
                def _():
                    inward(h, k, 1).wait_recv()

            query = query_in[h, pl.ds(b * WIDTH, WIDTH)].reshape(rows, lanes).astype(jnp.float32)
            both = jnp.concatenate(
                [jnp.where(in_first, query, 0.0), jnp.where(in_first, 0.0, query)], axis=0
            ).astype(half)
            keys = key_in[h].reshape(length, lanes)
            scores = lax.dot_general(
                both, keys, (((1,), (1,)), ((), ())), preferred_element_type=jnp.float32
            )
            one, two = part_of(scores[:rows]), part_of(scores[rows:])
            one_scale = 1.0 / jnp.sum(one, axis=-1, keepdims=True)
            two_scale = lambda_ref[h] / jnp.sum(two, axis=-1, keepdims=True)
            mixing = (one * one_scale - two * two_scale).astype(half)
            mixed = jnp.dot(
                mixing, value_in[h].reshape(length, lanes), preferred_element_type=jnp.float32
            )
            norm = lax.rsqrt(jnp.mean(mixed * mixed, axis=-1, keepdims=True) + 1e-05)
            result = (mixed * norm * head_gain_ref[...]).astype(half)
            head_out[h, pl.ds(b * WIDTH, WIDTH)] = result.reshape(WIDTH, tokens, lanes)
            for i in range(WIDTH):
                k = b * WIDTH + i

                @pl.when(k > 0)
                def _():
                    outward(h, k).start()

    for h in range(heads):
        token_rows[h, :, tile_of(me, lanes)] = head_out[h, 0]

    depth = count * lanes
    square_ref[...] = jnp.zeros_like(square_ref)

    def squares(value):
        value = value * value
        total = value[:, :128]
        for i in range(1, wide // 128):
            total = total + value[:, i * 128 : (i + 1) * 128]
        square_ref[...] += total

    def inverse_root():
        total = jnp.sum(square_ref[...], axis=-1, keepdims=True)
        return lax.rsqrt(total / model + 1e-06)

    for h in range(heads):

        @pl.loop(0, count)
        def _(o):
            weight_load(h, o).wait()

        @pl.loop(1, count)
        def _(k):
            outward(h, k).wait_recv()

        @pl.loop(0, model // wide)
        def _(n):
            cols = tile_of(n, wide)
            value = jnp.dot(
                token_rows[h], pool[h * depth : (h + 1) * depth, cols], preferred_element_type=jnp.float32
            )
            if h > 0:
                value = value + projected[:, cols]
            projected[:, cols] = value
            if h == heads - 1:
                squares(value)

    norm = inverse_root()
    square_ref[...] = jnp.zeros_like(square_ref)
    inputs[5].wait()

    @pl.loop(0, model // wide)
    def _(n):
        cols = tile_of(n, wide)
        stream = residual_ref[:, cols].astype(jnp.float32)
        stream = stream + projected[:, cols] * norm * mixer_gain_ref[:, cols]
        stream = stream.astype(half)
        stream_ref[:, cols] = stream
        squares(stream.astype(jnp.float32))

    norm2 = inverse_root()

    @pl.loop(0, model // wide)
    def _(n):
        cols = tile_of(n, wide)
        normed = stream_ref[:, cols].astype(jnp.float32) * norm2 * channel_gain_ref[:, cols]
        normed_ref[:, cols] = normed.astype(half)

    def send_out(k):
        return remote(outgoing.at[k], arrived.at[k, 0, 0], a_send.at[k], a_recv.at[k], sp_at(k))

    def cross_out(k, j):
        return remote(arrived.at[k, 0, 0], arrived.at[k, 0, j], b_send.at[k, j], b_recv.at[k, j], chip_at(j))

    def twin_out(k, j):
        return remote(arrived.at[k, 0, j], arrived.at[k, 1, j], c_send.at[k, j], c_recv.at[k, j], other)

    def pair_rows(k, j):
        return pl.ds(pl.multiple_of((k * groups + j) * capacity, capacity), capacity)

    def pair_out(k, j):
        return remote(arrived.at[k, 1, j], pool.at[pair_rows(k, j)], d_send.at[k, j], d_recv.at[k, j], other)

    def cross_back(k, j):
        return remote(own.at[k, j], cross_in.at[k, j - 1], e_send.at[k, j], e_recv.at[k, j], chip_at(-j))

    def send_back(k):
        return remote(own.at[k, 0], returned.at[k], f_send.at[k], f_recv.at[k], sp_at(k))

    near = count // 2

    def gather(first):
        @pl.loop(0, model // wide)
        def _(n):
            cols = tile_of(n, wide)
            chosen = place_ref[first * capacity : (first + near) * capacity, :]
            block = jnp.dot(chosen, normed_ref[:, cols], preferred_element_type=jnp.float32)
            block = block.astype(half).reshape(near, capacity, wide)
            outgoing[first : first + near, :, cols] = block
            if first == 0:
                arrived[0, 0, 0, :, cols] = block[0]

    gather(0)

    @pl.loop(1, near)
    def _(k):
        send_out(k).start()

    gather(near)

    @pl.loop(near, count)
    def _(k):
        send_out(k).start()

    def forward(k):
        @pl.when(k > 0)
        def _():
            send_out(k).wait_recv()

        for j in range(1, groups):
            cross_out(k, j).start()
        twin_out(k, 0).start()

    def forward_twin(k):
        for j in range(1, groups):
            cross_out(k, j).wait_recv()
            twin_out(k, j).start()

    def complete(k):
        for j in range(groups):
            twin_out(k, j).wait_recv()

    def pair_sum(k):
        for j in range(groups):
            pair_out(k, j).wait_recv()
            given = pool[pair_rows(k, j), :].astype(jnp.float32)
            own[k, j] = (own[k, j].astype(jnp.float32) + given).astype(half)
        for j in range(1, groups):
            cross_back(k, j).start()

    def total(k):
        value = own[k, 0].astype(jnp.float32)
        for j in range(1, groups):
            cross_back(k, j).wait_recv()
            value = value + cross_in[k, j - 1].astype(jnp.float32)
        value = value.astype(half)

        @pl.when(k > 0)
        def _():
            own[k, 0] = value
            send_back(k).start()

        @pl.when(k == 0)
        def _():
            returned[k] = value

    tile = math.gcd(units, 256)
    held = 2 * groups * capacity

    def compute(k):
        @pl.loop(0, units // tile)
        def _(n):
            cols = tile_of(n, tile)
            value = arrived[k].reshape(held, model)
            gate = jnp.dot(value, gate_w[:, cols], preferred_element_type=jnp.float32)
            up = jnp.dot(value, up_w[:, cols], preferred_element_type=jnp.float32)
            hidden[:, cols] = (gate / (1.0 + jnp.exp(-gate)) * up).astype(half)

        @pl.loop(0, model // wide)
        def _(n):
            cols = tile_of(n, wide)
            part = jnp.dot(hidden[...], down_w[:, cols], preferred_element_type=jnp.float32)
            part = part.astype(half).reshape(2, groups, capacity, wide)
            own[k, :, :, cols] = part[0]
            arrived[k, 1, :, :, cols] = part[1]

        for j in range(groups):
            pair_out(k, j).start()

    for copy in expert_loads:
        copy.wait()

    @pl.loop(0, count + 3)
    def _(g):
        @pl.when(g < count)
        def _():
            forward(g)

        @pl.when((g >= 2) & (g < count + 2))
        def _():
            pair_sum(g - 2)

        @pl.when(g >= 3)
        def _():
            total(g - 3)

        @pl.when((g >= 1) & (g < count + 1))
        def _():
            forward_twin(g - 1)
            complete(g - 1)
            compute(g - 1)

    square_ref[...] = jnp.zeros_like(square_ref)

    @pl.loop(1, count)
    def _(k):
        send_back(k).wait_recv()

    @pl.loop(0, model // wide)
    def _(n):
        cols = tile_of(n, wide)
        back = returned[:, :, cols].reshape(slots, wide)
        piece = jnp.dot(high_ref[...], back, preferred_element_type=jnp.float32)
        piece = piece + jnp.dot(low_ref[...], back, preferred_element_type=jnp.float32)
        projected[:, cols] = piece
        squares(piece)

    norm3 = inverse_root()

    def out_copy(n):
        cols = tile_of(n, wide)
        return pltpu.make_async_copy(normed_ref.at[:, cols], out_hbm.at[:, cols], out_sem.at[n])

    @pl.loop(0, model // wide)
    def _(n):
        cols = tile_of(n, wide)
        value = stream_ref[:, cols].astype(jnp.float32)
        value = value + projected[:, cols] * norm3 * expert_gain_ref[:, cols]
        normed_ref[:, cols] = value.astype(half)
        out_copy(n).start()

    for h in range(heads):

        @pl.loop(1, count)
        def _(k):
            for i in range(3):
                inward(h, k, i).wait_send()
            outward(h, k).wait_send()

    @pl.loop(0, count)
    def _(k):
        @pl.when(k > 0)
        def _():
            send_out(k).wait_send()
            send_back(k).wait_send()

        for j in range(1, groups):
            cross_out(k, j).wait_send()
            cross_back(k, j).wait_send()
        for j in range(groups):
            twin_out(k, j).wait_send()
            pair_out(k, j).wait_send()

    @pl.loop(0, model // wide)
    def _(n):
        out_copy(n).wait()


def local(
    queries,
    key_rows,
    value_rows,
    lambdas,
    head_gain,
    out_weight,
    residual,
    mixer_gain,
    channel_gain,
    expert_gain,
    routes,
    route_logits,
    gate_weight,
    up_weight,
    down_weight,
):
    count, groups = lax.axis_size("sp"), lax.axis_size("dp") // 2
    heads = lambdas.shape[0]
    lanes = head_gain.shape[0]
    map_dim = lanes // 2
    _, tokens, model = residual.shape
    units = gate_weight.shape[2]
    capacity = -(-max(2, 3 * tokens // count) // 16) * 16
    slots = count * capacity
    inverse = 1.0 / np.float32(10000.0) ** (np.arange(0, map_dim, 2, dtype=np.float32) / np.float32(map_dim))
    angles = np.arange(count * tokens, dtype=np.float32)[:, None] * inverse.astype(np.float32)[None, :]
    cosine = np.cos(angles.astype(np.float64)).astype(np.float32)
    sine = np.sin(angles.astype(np.float64)).astype(np.float32)
    cos_table = jnp.asarray(np.concatenate([cosine] * 4, axis=1))
    sin_table = jnp.asarray(np.concatenate([-sine, sine] * 2, axis=1))
    vmem = pl.BlockSpec(memory_space=pltpu.VMEM)
    smem = pl.BlockSpec(memory_space=pltpu.SMEM)
    anywhere = pl.BlockSpec(memory_space=pl.ANY)
    half = jnp.bfloat16
    dma = pltpu.SemaphoreType.DMA
    rows = pltpu.VMEM((tokens, model), half)
    blocks = pltpu.VMEM((heads, count, tokens, lanes), half)
    table = pltpu.VMEM((tokens, lanes), jnp.float32)
    pool_rows = max(out_weight.shape[0], slots * groups)
    wide = math.gcd(model, 512)
    updated = pl.pallas_call(
        functools.partial(layer_kernel, count, groups),
        out_shape=jax.ShapeDtypeStruct((tokens, model), half),
        in_specs=[anywhere] * 5 + [smem, vmem, anywhere] + [vmem] * 5 + [anywhere] * 4,
        out_specs=anywhere,
        scratch_shapes=[
            rows,
            rows,
            rows,
            table,
            table,
            rows,
            blocks,
            blocks,
            blocks,
            blocks,
            blocks,
            blocks,
            pltpu.VMEM((heads, tokens, count * lanes), half),
            pltpu.VMEM((tokens, model), jnp.float32),
            pltpu.VMEM((tokens, 128), jnp.float32),
            rows,
            rows,
            pltpu.VMEM((slots, tokens), half),
            pltpu.VMEM((tokens, slots), half),
            pltpu.VMEM((tokens, slots), half),
            pltpu.VMEM((pool_rows, model), half),
            pltpu.VMEM((count, capacity, model), half),
            pltpu.VMEM((count, 2, groups, capacity, model), half),
            pltpu.VMEM((count, groups, capacity, model), half),
            pltpu.VMEM((count, max(1, groups - 1), capacity, model), half),
            pltpu.VMEM((count, capacity, model), half),
            pltpu.VMEM((2 * groups * capacity, units), half),
            pltpu.VMEM((model, units), half),
            pltpu.VMEM((model, units), half),
            pltpu.VMEM((units, model), half),
            dma((6,)),
            dma((heads, count)),
            dma((3,)),
            dma((model // wide,)),
            dma((heads, 3, count)),
            dma((heads, 3, count)),
            dma((heads, count)),
            dma((heads, count)),
            dma((count,)),
            dma((count,)),
            dma((count, groups)),
            dma((count, groups)),
            dma((count, groups)),
            dma((count, groups)),
            dma((count, groups)),
            dma((count, groups)),
            dma((count, groups)),
            dma((count, groups)),
            dma((count,)),
            dma((count,)),
        ],
        compiler_params=pltpu.CompilerParams(
            collective_id=1, has_side_effects=True, vmem_limit_bytes=67043328
        ),
        name="layer",
    )(
        queries[0],
        key_rows[0],
        value_rows[0],
        cos_table,
        sin_table,
        lambdas,
        head_gain[None, :],
        residual[0],
        mixer_gain[None, :],
        channel_gain[None, :],
        expert_gain[None, :],
        routes[0].T,
        route_logits[0].T,
        out_weight,
        gate_weight[0],
        up_weight[0],
        down_weight[0],
    )
    return updated[None]


def solution(mesh):
    placed = (
        P("dp", "sp", None),
        P("dp", "sp", None),
        P("dp", "sp", None),
        P("sp"),
        P(),
        P(),
        P("dp", "sp", None),
        P(),
        P(),
        P(),
        P("dp", "sp", None),
        P("dp", "sp", None),
        P("sp", None, "dp"),
        P("sp", None, "dp"),
        P("sp", "dp", None),
    )
    return jax.shard_map(
        local, mesh=mesh, in_specs=placed, out_specs=P("dp", "sp", None), check_vma=False
    )
```

```python
import contextlib
import functools
import math

import jax
import jax.numpy as jnp
import numpy as np
from jax import lax
from jax.experimental import pallas as pl
from jax.experimental.pallas import tpu as pltpu
from jax.sharding import PartitionSpec as P


MESH = pl.DeviceIdType.MESH
WIDTH = 2
TRACE = False


def scope(name):
    return jax.named_scope(name) if TRACE else contextlib.nullcontext()


KINDS = "AYUDPT"
INNER = (
    "A1", "Y0", "U0", "D0", "A2", "Y1", "U1", "A4", "D1", "A3", "Y2", "U2", "Y4", "D2", "A5", "U4",
    "D4", "Y3", "P4", "Y5", "A6", "U5", "A7", "D5", "T4", "U3", "P5", "P1", "D3", "Y6", "U6", "D6",
    "T5", "P6", "P2", "Y7", "U7", "T6", "D7", "P7", "P3", "P0", "T1", "T2", "T7", "T3", "T0",
)
OUTER = (
    "A1", "Y0", "U0", "D0", "A2", "Y1", "U1", "A4", "D1", "A3", "Y2", "U2", "Y4", "P1", "D2", "U4",
    "A5", "D4", "Y3", "P4", "Y5", "U3", "A6", "D3", "U5", "T4", "D5", "A7", "P5", "Y6", "U6", "D6",
    "T5", "P6", "P2", "Y7", "U7", "D7", "T6", "P7", "P3", "P0", "T1", "T7", "T2", "T3", "T0",
)


def plan(count, eight):
    if count == 8:
        return [(KINDS.index(step[0]), int(step[1:])) for step in eight]
    steps = []
    for n in range(count + 3):
        if 0 < n < count:
            steps.append((KINDS.index("A"), n))
        if 2 <= n < count + 2:
            steps.append((KINDS.index("P"), n - 2))
        if n >= 3:
            steps.append((KINDS.index("T"), n - 3))
        if 1 <= n <= count:
            steps += [(KINDS.index(kind), n - 1) for kind in "YUD"]
    return steps


def layer_kernel(
    count,
    groups,
    query_hbm,
    key_hbm,
    value_hbm,
    cos_hbm,
    sin_hbm,
    lambda_ref,
    head_gain_ref,
    residual_hbm,
    mixer_gain_ref,
    channel_gain_ref,
    expert_gain_ref,
    routes_ref,
    logits_ref,
    weight_hbm,
    gate_hbm,
    up_hbm,
    down_hbm,
    out_hbm,
    query_ref,
    key_ref,
    value_ref,
    cos_ref,
    sin_ref,
    residual_ref,
    query_out,
    key_out,
    query_in,
    key_in,
    value_in,
    head_out,
    token_rows,
    projected,
    square_ref,
    stream_ref,
    normed_ref,
    place_ref,
    high_ref,
    low_ref,
    pool,
    outgoing,
    arrived,
    own,
    cross_in,
    returned,
    hidden,
    gate_w,
    up_w,
    down_w,
    in_sem,
    weight_sem,
    expert_sem,
    out_sem,
    in_send,
    in_recv,
    head_send,
    head_recv,
    a_send,
    a_recv,
    b_send,
    b_recv,
    c_send,
    c_recv,
    d_send,
    d_recv,
    e_send,
    e_recv,
    f_send,
    f_recv,
):
    me = lax.axis_index("sp")
    dp = lax.axis_index("dp")
    chip, core = dp // 2, dp % 2
    tokens, model = query_ref.shape
    lanes = head_gain_ref.shape[1]
    heads = lambda_ref.shape[0]
    map_dim = lanes // 2
    scale = map_dim ** (-0.5)
    capacity = outgoing.shape[1]
    units = gate_w.shape[1]
    wide = math.gcd(model, 512)
    half = jnp.bfloat16

    def peer(k):
        total, bit = 0, 1
        while bit < count:
            a, b = (me // bit) % 2, (k // bit) % 2
            total = total + bit * (a + b - 2 * a * b)
            bit *= 2
        return total

    other = {"sp": me, "dp": chip * 2 + (1 - core)}

    def chip_at(step):
        return {"sp": me, "dp": ((chip + step + groups) % groups) * 2 + core}

    def sp_at(k):
        return {"sp": peer(k), "dp": dp}

    def columns(owner, h):
        return pl.ds(pl.multiple_of((owner * heads + h) * lanes, lanes), lanes)

    def tile_of(n, size):
        return pl.ds(pl.multiple_of(n * size, size), size)

    def remote(src, dst, send, recv, device):
        return pltpu.make_async_remote_copy(
            src_ref=src, dst_ref=dst, send_sem=send, recv_sem=recv, device_id=device, device_id_type=MESH
        )

    rows_here = pl.ds(pl.multiple_of(me * tokens, tokens), tokens)
    inputs = [
        pltpu.make_async_copy(src, dst, in_sem.at[i])
        for i, (src, dst) in enumerate(
            (
                (value_hbm, value_ref),
                (key_hbm, key_ref),
                (cos_hbm.at[rows_here], cos_ref),
                (sin_hbm.at[rows_here], sin_ref),
                (query_hbm, query_ref),
                (residual_hbm, residual_ref),
            )
        )
    ]
    for copy in inputs:
        copy.start()

    def weight_load(h, o):
        return pltpu.make_async_copy(
            weight_hbm.at[columns(o, h)],
            pool.at[pl.ds(pl.multiple_of((h * count + o) * lanes, lanes), lanes)],
            weight_sem.at[h, o],
        )

    expert_loads = [
        pltpu.make_async_copy(src, dst, expert_sem.at[i])
        for i, (src, dst) in enumerate(((gate_hbm, gate_w), (up_hbm, up_w), (down_hbm, down_w)))
    ]

    barrier = pltpu.get_barrier_semaphore()
    peers = [sp_at(k) for k in range(1, count)] + [chip_at(j) for j in range(1, groups)] + [other]
    for device in peers:
        pl.semaphore_signal(barrier, inc=1, device_id=device, device_id_type=MESH)

    def inward(h, k, i):
        sources = (value_ref.at[:, columns(peer(k), h)], query_out.at[h, k], key_out.at[h, k])
        targets = (value_in.at[h, k], query_in.at[h, k], key_in.at[h, k])
        return remote(sources[i], targets[i], in_send.at[h, i, k], in_recv.at[h, i, k], sp_at(k))

    def outward(h, k):
        return remote(
            head_out.at[h, k],
            token_rows.at[h, :, tile_of(me, lanes)],
            head_send.at[h, k],
            head_recv.at[h, k],
            sp_at(k),
        )

    first_half = lax.broadcasted_iota(jnp.int32, (tokens, lanes), 1) % map_dim < map_dim // 2

    def turned(ref, cols):
        x = ref[:, cols].astype(jnp.float32)
        ahead = pltpu.roll(x, lanes - map_dim // 2, 1)
        behind = pltpu.roll(x, map_dim // 2, 1)
        return x * cos_ref[...] + jnp.where(first_half, ahead, behind) * sin_ref[...]

    def turned_query(cols):
        return (turned(query_ref, cols) * scale).astype(half)

    def turned_key(cols):
        return turned(key_ref, cols).astype(half)

    with scope("barrier"):
        inputs[0].wait()
        pl.semaphore_wait(barrier, len(peers))

    with scope("prepare"):
        for h in range(heads):

            @pl.loop(1, count)
            def _(k):
                inward(h, k, 0).start()

            if h == 0:
                for copy in inputs[1:4]:
                    copy.wait()

            @pl.loop(1, count)
            def _(k):
                key_out[h, k] = turned_key(columns(peer(k), h))

            @pl.loop(1, count)
            def _(k):
                inward(h, k, 2).start()

            if h == 0:
                inputs[4].wait()

            @pl.loop(1, count)
            def _(k):
                query_out[h, k] = turned_query(columns(peer(k), h))

            @pl.loop(1, count)
            def _(k):
                inward(h, count - k, 1).start()

        for h in range(heads):
            query_in[h, 0] = turned_query(columns(me, h))
            key_in[h, 0] = turned_key(columns(me, h))
            value_in[h, 0] = value_ref[:, columns(me, h)]

        for h in range(heads):

            @pl.loop(0, count)
            def _(o):
                weight_load(h, o).start()

        for copy in expert_loads:
            copy.start()

    with scope("routing"):
        top = routes_ref.shape[0]
        slots = count * capacity
        ranks = max(16, count)
        experts = lax.broadcasted_iota(jnp.int32, (ranks, tokens), 0)
        places = lax.broadcasted_iota(jnp.int32, (slots, tokens), 0)
        upper = lax.broadcasted_iota(jnp.int32, (tokens, tokens), 0)
        upper = (upper <= lax.broadcasted_iota(jnp.int32, (tokens, tokens), 1)).astype(half)
        logits = logits_ref[...]
        odds = jnp.exp(logits - jnp.max(logits, axis=0, keepdims=True))
        shares = odds / jnp.sum(odds, axis=0, keepdims=True)
        used = jnp.zeros((ranks, 1), jnp.float32)
        mix = jnp.zeros((slots, tokens), jnp.float32)
        place = jnp.zeros((slots, tokens), jnp.float32)
        for i in range(top):
            ranked = jnp.bitwise_xor(routes_ref[i : i + 1, :], me)
            named = (experts == ranked).astype(jnp.float32)
            running = jnp.dot(named.astype(half), upper, preferred_element_type=jnp.float32)
            slot = jnp.sum(named * (running + used), axis=0, keepdims=True).astype(jnp.int32) - 1
            used = used + jnp.sum(named, axis=1, keepdims=True)
            hit = places == ranked * capacity + slot
            mix = mix + jnp.where(hit, shares[i : i + 1, :], 0.0)
            place = place + jnp.where(hit, 1.0, 0.0)
        place_ref[...] = place.astype(half)
        mix = mix.T
        high = mix.astype(half)
        high_ref[...] = high
        low_ref[...] = (mix - high.astype(jnp.float32)).astype(half)

    rows = WIDTH * tokens
    length = count * tokens
    in_first = lax.broadcasted_iota(jnp.int32, (rows, lanes), 1) < map_dim

    def part_of(total):
        return jnp.exp(total - jnp.max(total, axis=-1, keepdims=True))

    for h in range(heads):

        with scope("wait_kv"):
            @pl.loop(1, count)
            def _(k):
                inward(h, k, 0).wait_recv()
                inward(h, k, 2).wait_recv()

        @pl.loop(0, count // WIDTH)
        def _(step):
            b = count // WIDTH - 1 - step
            with scope("wait_q"):
                for i in range(WIDTH):
                    k = b * WIDTH + i

                    @pl.when(k > 0)
                    def _():
                        inward(h, k, 1).wait_recv()

            with scope("attend"):
                query = query_in[h, pl.ds(b * WIDTH, WIDTH)].reshape(rows, lanes).astype(jnp.float32)
                both = jnp.concatenate(
                    [jnp.where(in_first, query, 0.0), jnp.where(in_first, 0.0, query)], axis=0
                ).astype(half)
                keys = key_in[h].reshape(length, lanes)
                scores = lax.dot_general(
                    both, keys, (((1,), (1,)), ((), ())), preferred_element_type=jnp.float32
                )
                one, two = part_of(scores[:rows]), part_of(scores[rows:])
                one_scale = 1.0 / jnp.sum(one, axis=-1, keepdims=True)
                two_scale = lambda_ref[h] / jnp.sum(two, axis=-1, keepdims=True)
                mixing = (one * one_scale - two * two_scale).astype(half)
                mixed = jnp.dot(
                    mixing, value_in[h].reshape(length, lanes), preferred_element_type=jnp.float32
                )
                norm = lax.rsqrt(jnp.mean(mixed * mixed, axis=-1, keepdims=True) + 1e-05)
                result = (mixed * norm * head_gain_ref[...]).astype(half)
                head_out[h, pl.ds(b * WIDTH, WIDTH)] = result.reshape(WIDTH, tokens, lanes)
            for i in range(WIDTH):
                k = b * WIDTH + i

                @pl.when(k > 0)
                def _():
                    outward(h, k).start()

    for h in range(heads):
        token_rows[h, :, tile_of(me, lanes)] = head_out[h, 0]

    depth = count * lanes
    square_ref[...] = jnp.zeros_like(square_ref)

    def squares(value):
        value = value * value
        total = value[:, :128]
        for i in range(1, wide // 128):
            total = total + value[:, i * 128 : (i + 1) * 128]
        square_ref[...] += total

    def inverse_root():
        total = jnp.sum(square_ref[...], axis=-1, keepdims=True)
        return lax.rsqrt(total / model + 1e-06)

    for h in range(heads):

        @pl.loop(0, count)
        def _(o):
            weight_load(h, o).wait()

        with scope("wait_heads"):
            @pl.loop(1, count)
            def _(k):
                outward(h, k).wait_recv()

        with scope("project"):
            @pl.loop(0, model // wide)
            def _(n):
                cols = tile_of(n, wide)
                value = jnp.dot(
                    token_rows[h], pool[h * depth : (h + 1) * depth, cols], preferred_element_type=jnp.float32
                )
                if h > 0:
                    value = value + projected[:, cols]
                projected[:, cols] = value
                if h == heads - 1:
                    squares(value)

    with scope("norms"):
        norm = inverse_root()
        square_ref[...] = jnp.zeros_like(square_ref)
        inputs[5].wait()

        @pl.loop(0, model // wide)
        def _(n):
            cols = tile_of(n, wide)
            stream = residual_ref[:, cols].astype(jnp.float32)
            stream = stream + projected[:, cols] * norm * mixer_gain_ref[:, cols]
            stream = stream.astype(half)
            stream_ref[:, cols] = stream
            squares(stream.astype(jnp.float32))

        norm2 = inverse_root()

        @pl.loop(0, model // wide)
        def _(n):
            cols = tile_of(n, wide)
            normed = stream_ref[:, cols].astype(jnp.float32) * norm2 * channel_gain_ref[:, cols]
            normed_ref[:, cols] = normed.astype(half)

    def send_out(k):
        return remote(outgoing.at[k], arrived.at[k, 0, 0], a_send.at[k], a_recv.at[k], sp_at(k))

    def cross_out(k, j):
        return remote(arrived.at[k, 0, 0], arrived.at[k, 0, j], b_send.at[k, j], b_recv.at[k, j], chip_at(j))

    def twin_out(k, j):
        return remote(arrived.at[k, 0, j], arrived.at[k, 1, j], c_send.at[k, j], c_recv.at[k, j], other)

    def pair_rows(k, j):
        return pl.ds(pl.multiple_of((k * groups + j) * capacity, capacity), capacity)

    def pair_out(k, j):
        return remote(arrived.at[k, 1, j], pool.at[pair_rows(k, j)], d_send.at[k, j], d_recv.at[k, j], other)

    def cross_back(k, j):
        return remote(own.at[k, j], cross_in.at[k, j - 1], e_send.at[k, j], e_recv.at[k, j], chip_at(-j))

    def send_back(k):
        return remote(own.at[k, 0], returned.at[k], f_send.at[k], f_recv.at[k], sp_at(k))

    near = count // 2

    def gather(first):
        @pl.loop(0, model // wide)
        def _(n):
            cols = tile_of(n, wide)
            chosen = place_ref[first * capacity : (first + near) * capacity, :]
            block = jnp.dot(chosen, normed_ref[:, cols], preferred_element_type=jnp.float32)
            block = block.astype(half).reshape(near, capacity, wide)
            outgoing[first : first + near, :, cols] = block
            if first == 0:
                arrived[0, 0, 0, :, cols] = block[0]

    def forward(k):
        @pl.when(k > 0)
        def _():
            with scope("A_wait"):
                send_out(k).wait_recv()

        for j in range(1, groups):
            cross_out(k, j).start()
        twin_out(k, 0).start()

    with scope("gather"):
        gather(0)

        @pl.loop(1, near)
        def _(k):
            send_out(k).start()

        forward(0)
        gather(near)

        @pl.loop(near, count)
        def _(k):
            send_out(k).start()

    def forward_twin(k):
        for j in range(1, groups):
            with scope("Y_wait"):
                cross_out(k, j).wait_recv()
            twin_out(k, j).start()

    def complete(k):
        for j in range(groups):
            with scope("twin_wait"):
                twin_out(k, j).wait_recv()

    def pair_sum(k):
        for j in range(groups):
            with scope("pair_wait"):
                pair_out(k, j).wait_recv()
            given = pool[pair_rows(k, j), :].astype(jnp.float32)
            own[k, j] = (own[k, j].astype(jnp.float32) + given).astype(half)
        for j in range(1, groups):
            cross_back(k, j).start()

    def total(k):
        value = own[k, 0].astype(jnp.float32)
        for j in range(1, groups):
            with scope("B_wait"):
                cross_back(k, j).wait_recv()
            value = value + cross_in[k, j - 1].astype(jnp.float32)
        value = value.astype(half)

        @pl.when(k > 0)
        def _():
            own[k, 0] = value
            send_back(k).start()

        @pl.when(k == 0)
        def _():
            returned[k] = value

    tile = math.gcd(units, 256)
    held = 2 * groups * capacity

    def expand(k):
        complete(k)

        with scope("ffn_up"):
            @pl.loop(0, units // tile)
            def _(n):
                cols = tile_of(n, tile)
                value = arrived[k].reshape(held, model)
                gate = jnp.dot(value, gate_w[:, cols], preferred_element_type=jnp.float32)
                up = jnp.dot(value, up_w[:, cols], preferred_element_type=jnp.float32)
                hidden[:, cols] = (gate / (1.0 + jnp.exp(-gate)) * up).astype(half)

    def contract(k):
        with scope("ffn_down"):
            @pl.loop(0, model // wide)
            def _(n):
                cols = tile_of(n, wide)
                part = jnp.dot(hidden[...], down_w[:, cols], preferred_element_type=jnp.float32)
                part = part.astype(half).reshape(2, groups, capacity, wide)
                own[k, :, :, cols] = part[0]
                arrived[k, 1, :, :, cols] = part[1]

        for j in range(groups):
            pair_out(k, j).start()

    for copy in expert_loads:
        copy.wait()

    kinds = (forward, forward_twin, expand, contract, pair_sum, total)
    inner, outer = ([kind * count + k for kind, k in plan(count, eight)] for eight in (INNER, OUTER))
    ends = (me < count // 4) | (me >= count - count // 4)

    @pl.loop(0, len(inner))
    def _(i):
        code = 0
        for n in range(len(inner)):
            value = inner[n] if inner[n] == outer[n] else jnp.where(ends, outer[n], inner[n])
            code = jnp.where(i == n, value, code)
        for kind, action in enumerate(kinds):

            @pl.when(code // count == kind)
            def _():
                action(code % count)

    square_ref[...] = jnp.zeros_like(square_ref)

    with scope("wait_back"):
        @pl.loop(1, count)
        def _(k):
            send_back(k).wait_recv()

    with scope("combine"):
        @pl.loop(0, model // wide)
        def _(n):
            cols = tile_of(n, wide)
            back = returned[:, :, cols].reshape(slots, wide)
            piece = jnp.dot(high_ref[...], back, preferred_element_type=jnp.float32)
            piece = piece + jnp.dot(low_ref[...], back, preferred_element_type=jnp.float32)
            projected[:, cols] = piece
            squares(piece)

        norm3 = inverse_root()

        def out_copy(n):
            cols = tile_of(n, wide)
            return pltpu.make_async_copy(normed_ref.at[:, cols], out_hbm.at[:, cols], out_sem.at[n])

        @pl.loop(0, model // wide)
        def _(n):
            cols = tile_of(n, wide)
            value = stream_ref[:, cols].astype(jnp.float32)
            value = value + projected[:, cols] * norm3 * expert_gain_ref[:, cols]
            normed_ref[:, cols] = value.astype(half)
            out_copy(n).start()

    with scope("drain"):
        for h in range(heads):

            @pl.loop(1, count)
            def _(k):
                for i in range(3):
                    inward(h, k, i).wait_send()
                outward(h, k).wait_send()

        @pl.loop(0, count)
        def _(k):
            @pl.when(k > 0)
            def _():
                send_out(k).wait_send()
                send_back(k).wait_send()

            for j in range(1, groups):
                cross_out(k, j).wait_send()
                cross_back(k, j).wait_send()
            for j in range(groups):
                twin_out(k, j).wait_send()
                pair_out(k, j).wait_send()

        @pl.loop(0, model // wide)
        def _(n):
            out_copy(n).wait()


def local(
    queries,
    key_rows,
    value_rows,
    lambdas,
    head_gain,
    out_weight,
    residual,
    mixer_gain,
    channel_gain,
    expert_gain,
    routes,
    route_logits,
    gate_weight,
    up_weight,
    down_weight,
):
    count, groups = lax.axis_size("sp"), lax.axis_size("dp") // 2
    heads = lambdas.shape[0]
    lanes = head_gain.shape[0]
    map_dim = lanes // 2
    _, tokens, model = residual.shape
    units = gate_weight.shape[2]
    capacity = -(-max(2, 3 * tokens // count) // 16) * 16
    slots = count * capacity
    inverse = 1.0 / np.float32(10000.0) ** (np.arange(0, map_dim, 2, dtype=np.float32) / np.float32(map_dim))
    angles = np.arange(count * tokens, dtype=np.float32)[:, None] * inverse.astype(np.float32)[None, :]
    cosine = np.cos(angles.astype(np.float64)).astype(np.float32)
    sine = np.sin(angles.astype(np.float64)).astype(np.float32)
    cos_table = jnp.asarray(np.concatenate([cosine] * 4, axis=1))
    sin_table = jnp.asarray(np.concatenate([-sine, sine] * 2, axis=1))
    vmem = pl.BlockSpec(memory_space=pltpu.VMEM)
    smem = pl.BlockSpec(memory_space=pltpu.SMEM)
    anywhere = pl.BlockSpec(memory_space=pl.ANY)
    half = jnp.bfloat16
    dma = pltpu.SemaphoreType.DMA
    rows = pltpu.VMEM((tokens, model), half)
    blocks = pltpu.VMEM((heads, count, tokens, lanes), half)
    table = pltpu.VMEM((tokens, lanes), jnp.float32)
    pool_rows = max(out_weight.shape[0], slots * groups)
    wide = math.gcd(model, 512)
    updated = pl.pallas_call(
        functools.partial(layer_kernel, count, groups),
        out_shape=jax.ShapeDtypeStruct((tokens, model), half),
        in_specs=[anywhere] * 5 + [smem, vmem, anywhere] + [vmem] * 5 + [anywhere] * 4,
        out_specs=anywhere,
        scratch_shapes=[
            rows,
            rows,
            rows,
            table,
            table,
            rows,
            blocks,
            blocks,
            blocks,
            blocks,
            blocks,
            blocks,
            pltpu.VMEM((heads, tokens, count * lanes), half),
            pltpu.VMEM((tokens, model), jnp.float32),
            pltpu.VMEM((tokens, 128), jnp.float32),
            rows,
            rows,
            pltpu.VMEM((slots, tokens), half),
            pltpu.VMEM((tokens, slots), half),
            pltpu.VMEM((tokens, slots), half),
            pltpu.VMEM((pool_rows, model), half),
            pltpu.VMEM((count, capacity, model), half),
            pltpu.VMEM((count, 2, groups, capacity, model), half),
            pltpu.VMEM((count, groups, capacity, model), half),
            pltpu.VMEM((count, max(1, groups - 1), capacity, model), half),
            pltpu.VMEM((count, capacity, model), half),
            pltpu.VMEM((2 * groups * capacity, units), half),
            pltpu.VMEM((model, units), half),
            pltpu.VMEM((model, units), half),
            pltpu.VMEM((units, model), half),
            dma((6,)),
            dma((heads, count)),
            dma((3,)),
            dma((model // wide,)),
            dma((heads, 3, count)),
            dma((heads, 3, count)),
            dma((heads, count)),
            dma((heads, count)),
            dma((count,)),
            dma((count,)),
            dma((count, groups)),
            dma((count, groups)),
            dma((count, groups)),
            dma((count, groups)),
            dma((count, groups)),
            dma((count, groups)),
            dma((count, groups)),
            dma((count, groups)),
            dma((count,)),
            dma((count,)),
        ],
        compiler_params=pltpu.CompilerParams(
            collective_id=1, has_side_effects=True, vmem_limit_bytes=67043328
        ),
        name="layer",
    )(
        queries[0],
        key_rows[0],
        value_rows[0],
        cos_table,
        sin_table,
        lambdas,
        head_gain[None, :],
        residual[0],
        mixer_gain[None, :],
        channel_gain[None, :],
        expert_gain[None, :],
        routes[0].T,
        route_logits[0].T,
        out_weight,
        gate_weight[0],
        up_weight[0],
        down_weight[0],
    )
    return updated[None]


def solution(mesh):
    placed = (
        P("dp", "sp", None),
        P("dp", "sp", None),
        P("dp", "sp", None),
        P("sp"),
        P(),
        P(),
        P("dp", "sp", None),
        P(),
        P(),
        P(),
        P("dp", "sp", None),
        P("dp", "sp", None),
        P("sp", None, "dp"),
        P("sp", None, "dp"),
        P("sp", "dp", None),
    )
    return jax.shard_map(
        local, mesh=mesh, in_specs=placed, out_specs=P("dp", "sp", None), check_vma=False
    )
```

```python
import contextlib
import functools
import math

import jax
import jax.numpy as jnp
import numpy as np
from jax import lax
from jax.experimental import pallas as pl
from jax.experimental.pallas import tpu as pltpu
from jax.sharding import PartitionSpec as P


MESH = pl.DeviceIdType.MESH
WIDTH = 2
TRACE = False


def scope(name):
    return jax.named_scope(name) if TRACE else contextlib.nullcontext()


KINDS = "AYUDPT"
INNER = (
    "A1", "Y0", "U0", "D0", "A2", "Y1", "U1", "A4", "D1", "A3", "Y2", "U2", "Y4", "D2", "A5", "U4",
    "D4", "Y3", "P4", "Y5", "A6", "U5", "A7", "D5", "T4", "U3", "P5", "P1", "D3", "Y6", "U6", "D6",
    "T5", "P6", "P2", "Y7", "U7", "T6", "D7", "P7", "P3", "P0", "T1", "T2", "T7", "T3", "T0",
)
OUTER = (
    "A1", "Y0", "U0", "D0", "A2", "Y1", "U1", "A4", "D1", "A3", "Y2", "U2", "Y4", "P1", "D2", "U4",
    "A5", "D4", "Y3", "P4", "Y5", "U3", "A6", "D3", "U5", "T4", "D5", "A7", "P5", "Y6", "U6", "D6",
    "T5", "P6", "P2", "Y7", "U7", "D7", "T6", "P7", "P3", "P0", "T1", "T7", "T2", "T3", "T0",
)


def plan(count, eight):
    if count == 8:
        return [(KINDS.index(step[0]), int(step[1:])) for step in eight]
    steps = []
    for n in range(count + 3):
        if 0 < n < count:
            steps.append((KINDS.index("A"), n))
        if 2 <= n < count + 2:
            steps.append((KINDS.index("P"), n - 2))
        if n >= 3:
            steps.append((KINDS.index("T"), n - 3))
        if 1 <= n <= count:
            steps += [(KINDS.index(kind), n - 1) for kind in "YUD"]
    return steps


def layer_kernel(
    count,
    groups,
    query_hbm,
    key_hbm,
    value_hbm,
    cos_hbm,
    sin_hbm,
    lambda_ref,
    head_gain_ref,
    residual_hbm,
    mixer_gain_ref,
    channel_gain_ref,
    expert_gain_ref,
    routes_ref,
    logits_ref,
    weight_hbm,
    gate_hbm,
    up_hbm,
    down_hbm,
    out_hbm,
    query_ref,
    key_ref,
    value_ref,
    cos_ref,
    sin_ref,
    residual_ref,
    query_out,
    key_out,
    query_in,
    key_in,
    value_in,
    head_out,
    token_rows,
    projected,
    square_ref,
    stream_ref,
    normed_ref,
    place_ref,
    high_ref,
    low_ref,
    pool,
    outgoing,
    arrived,
    own,
    cross_in,
    returned,
    hidden,
    gate_w,
    up_w,
    down_w,
    in_sem,
    weight_sem,
    expert_sem,
    out_sem,
    in_send,
    kv_recv,
    query_recv,
    head_send,
    head_recv,
    a_send,
    a_recv,
    b_send,
    b_recv,
    c_send,
    c_recv,
    d_send,
    d_recv,
    e_send,
    e_recv,
    f_send,
    f_recv,
):
    me = lax.axis_index("sp")
    dp = lax.axis_index("dp")
    chip, core = dp // 2, dp % 2
    tokens, model = query_ref.shape
    lanes = head_gain_ref.shape[1]
    heads = lambda_ref.shape[0]
    map_dim = lanes // 2
    scale = map_dim ** (-0.5)
    capacity = outgoing.shape[1]
    units = gate_w.shape[1]
    wide = math.gcd(model, 512)
    half = jnp.bfloat16

    def peer(k):
        total, bit = 0, 1
        while bit < count:
            a, b = (me // bit) % 2, (k // bit) % 2
            total = total + bit * (a + b - 2 * a * b)
            bit *= 2
        return total

    other = {"sp": me, "dp": chip * 2 + (1 - core)}

    def chip_at(step):
        return {"sp": me, "dp": ((chip + step + groups) % groups) * 2 + core}

    def sp_at(k):
        return {"sp": peer(k), "dp": dp}

    def columns(owner, h):
        return pl.ds(pl.multiple_of((owner * heads + h) * lanes, lanes), lanes)

    def tile_of(n, size):
        return pl.ds(pl.multiple_of(n * size, size), size)

    def remote(src, dst, send, recv, device):
        return pltpu.make_async_remote_copy(
            src_ref=src, dst_ref=dst, send_sem=send, recv_sem=recv, device_id=device, device_id_type=MESH
        )

    rows_here = pl.ds(pl.multiple_of(me * tokens, tokens), tokens)
    inputs = [
        pltpu.make_async_copy(src, dst, in_sem.at[i])
        for i, (src, dst) in enumerate(
            (
                (value_hbm, value_ref),
                (key_hbm, key_ref),
                (cos_hbm.at[rows_here], cos_ref),
                (sin_hbm.at[rows_here], sin_ref),
                (query_hbm, query_ref),
                (residual_hbm, residual_ref),
            )
        )
    ]
    for copy in inputs:
        copy.start()

    def weight_load(h, o):
        return pltpu.make_async_copy(
            weight_hbm.at[columns(o, h)],
            pool.at[pl.ds(pl.multiple_of((h * count + o) * lanes, lanes), lanes)],
            weight_sem.at[h],
        )

    expert_loads = [
        pltpu.make_async_copy(src, dst, expert_sem.at[i])
        for i, (src, dst) in enumerate(((gate_hbm, gate_w), (up_hbm, up_w), (down_hbm, down_w)))
    ]

    barrier = pltpu.get_barrier_semaphore()
    peers = [sp_at(k) for k in range(1, count)] + [chip_at(j) for j in range(1, groups)] + [other]
    for device in peers:
        pl.semaphore_signal(barrier, inc=1, device_id=device, device_id_type=MESH)

    def wait_bytes(ref, sem):
        pltpu.make_async_copy(ref, ref, sem).wait()

    def inward(h, k, i):
        sources = (value_ref.at[:, columns(peer(k), h)], query_out.at[h, k], key_out.at[h, k])
        targets = (value_in.at[h, k], query_in.at[h, k], key_in.at[h, k])
        landed = (kv_recv.at[h, 0], query_recv.at[h, k // WIDTH], kv_recv.at[h, 1])
        return remote(sources[i], targets[i], in_send.at[h, i], landed[i], sp_at(k))

    def outward(h, k):
        return remote(
            head_out.at[h, k],
            token_rows.at[h, :, tile_of(me, lanes)],
            head_send.at[h],
            head_recv.at[h, k],
            sp_at(k),
        )

    first_half = lax.broadcasted_iota(jnp.int32, (tokens, lanes), 1) % map_dim < map_dim // 2

    def turned(ref, cols):
        x = ref[:, cols].astype(jnp.float32)
        ahead = pltpu.roll(x, lanes - map_dim // 2, 1)
        behind = pltpu.roll(x, map_dim // 2, 1)
        return x * cos_ref[...] + jnp.where(first_half, ahead, behind) * sin_ref[...]

    def turned_query(cols):
        return (turned(query_ref, cols) * scale).astype(half)

    def turned_key(cols):
        return turned(key_ref, cols).astype(half)

    with scope("barrier"):
        inputs[0].wait()
        pl.semaphore_wait(barrier, len(peers))

    with scope("prepare"):
        for h in range(heads):

            @pl.loop(1, count)
            def _(k):
                inward(h, k, 0).start()

            if h == 0:
                for copy in inputs[1:4]:
                    copy.wait()

            @pl.loop(1, count)
            def _(k):
                key_out[h, k] = turned_key(columns(peer(k), h))

            @pl.loop(1, count)
            def _(k):
                inward(h, k, 2).start()

            if h == 0:
                inputs[4].wait()

            @pl.loop(1, count)
            def _(k):
                query_out[h, k] = turned_query(columns(peer(k), h))

            @pl.loop(1, count)
            def _(k):
                inward(h, count - k, 1).start()

        for h in range(heads):
            query_in[h, 0] = turned_query(columns(me, h))
            key_in[h, 0] = turned_key(columns(me, h))
            value_in[h, 0] = value_ref[:, columns(me, h)]

        for h in range(heads):

            @pl.loop(0, count)
            def _(o):
                weight_load(h, o).start()

        for copy in expert_loads:
            copy.start()

    with scope("routing"):
        top = routes_ref.shape[0]
        slots = count * capacity
        ranks = max(16, count)
        experts = lax.broadcasted_iota(jnp.int32, (ranks, tokens), 0)
        places = lax.broadcasted_iota(jnp.int32, (slots, tokens), 0)
        upper = lax.broadcasted_iota(jnp.int32, (tokens, tokens), 0)
        upper = (upper <= lax.broadcasted_iota(jnp.int32, (tokens, tokens), 1)).astype(half)
        logits = logits_ref[...]
        odds = jnp.exp(logits - jnp.max(logits, axis=0, keepdims=True))
        shares = odds / jnp.sum(odds, axis=0, keepdims=True)
        used = jnp.zeros((ranks, 1), jnp.float32)
        mix = jnp.zeros((slots, tokens), jnp.float32)
        place = jnp.zeros((slots, tokens), jnp.float32)
        for i in range(top):
            ranked = jnp.bitwise_xor(routes_ref[i : i + 1, :], me)
            named = (experts == ranked).astype(jnp.float32)
            running = jnp.dot(named.astype(half), upper, preferred_element_type=jnp.float32)
            slot = jnp.sum(named * (running + used), axis=0, keepdims=True).astype(jnp.int32) - 1
            used = used + jnp.sum(named, axis=1, keepdims=True)
            hit = places == ranked * capacity + slot
            mix = mix + jnp.where(hit, shares[i : i + 1, :], 0.0)
            place = place + jnp.where(hit, 1.0, 0.0)
        place_ref[...] = place.astype(half)
        mix = mix.T
        high = mix.astype(half)
        high_ref[...] = high
        low_ref[...] = (mix - high.astype(jnp.float32)).astype(half)

    rows = WIDTH * tokens
    length = count * tokens
    in_first = lax.broadcasted_iota(jnp.int32, (rows, lanes), 1) < map_dim

    def part_of(total):
        return jnp.exp(total - jnp.max(total, axis=-1, keepdims=True))

    for h in range(heads):

        with scope("wait_kv"):
            wait_bytes(value_in.at[h, 1:count], kv_recv.at[h, 0])
            wait_bytes(key_in.at[h, 1:count], kv_recv.at[h, 1])

        @pl.loop(0, count // WIDTH)
        def _(step):
            b = count // WIDTH - 1 - step
            with scope("wait_q"):
                @pl.when(b > 0)
                def _():
                    wait_bytes(query_in.at[h, pl.ds(b * WIDTH, WIDTH)], query_recv.at[h, b])

                @pl.when(b == 0)
                def _():
                    wait_bytes(query_in.at[h, 1:WIDTH], query_recv.at[h, b])

            with scope("attend"):
                query = query_in[h, pl.ds(b * WIDTH, WIDTH)].reshape(rows, lanes).astype(jnp.float32)
                both = jnp.concatenate(
                    [jnp.where(in_first, query, 0.0), jnp.where(in_first, 0.0, query)], axis=0
                ).astype(half)
                keys = key_in[h].reshape(length, lanes)
                scores = lax.dot_general(
                    both, keys, (((1,), (1,)), ((), ())), preferred_element_type=jnp.float32
                )
                one, two = part_of(scores[:rows]), part_of(scores[rows:])
                one_scale = 1.0 / jnp.sum(one, axis=-1, keepdims=True)
                two_scale = lambda_ref[h] / jnp.sum(two, axis=-1, keepdims=True)
                mixing = (one * one_scale - two * two_scale).astype(half)
                mixed = jnp.dot(
                    mixing, value_in[h].reshape(length, lanes), preferred_element_type=jnp.float32
                )
                norm = lax.rsqrt(jnp.mean(mixed * mixed, axis=-1, keepdims=True) + 1e-05)
                result = (mixed * norm * head_gain_ref[...]).astype(half)
                head_out[h, pl.ds(b * WIDTH, WIDTH)] = result.reshape(WIDTH, tokens, lanes)
            for i in range(WIDTH):
                k = b * WIDTH + i

                @pl.when(k > 0)
                def _():
                    outward(h, k).start()

    for h in range(heads):
        token_rows[h, :, tile_of(me, lanes)] = head_out[h, 0]

    depth = count * lanes
    square_ref[...] = jnp.zeros_like(square_ref)

    def squares(value):
        value = value * value
        total = value[:, :128]
        for i in range(1, wide // 128):
            total = total + value[:, i * 128 : (i + 1) * 128]
        square_ref[...] += total

    def inverse_root():
        total = jnp.sum(square_ref[...], axis=-1, keepdims=True)
        return lax.rsqrt(total / model + 1e-06)

    for h in range(heads):

        wait_bytes(pool.at[h * depth : (h + 1) * depth], weight_sem.at[h])

        with scope("wait_heads"):
            @pl.loop(1, count)
            def _(k):
                outward(h, k).wait_recv()

        with scope("project"):
            @pl.loop(0, model // wide)
            def _(n):
                cols = tile_of(n, wide)
                value = jnp.dot(
                    token_rows[h], pool[h * depth : (h + 1) * depth, cols], preferred_element_type=jnp.float32
                )
                if h > 0:
                    value = value + projected[:, cols]
                projected[:, cols] = value
                if h == heads - 1:
                    squares(value)

    with scope("norms"):
        norm = inverse_root()
        square_ref[...] = jnp.zeros_like(square_ref)
        inputs[5].wait()

        @pl.loop(0, model // wide)
        def _(n):
            cols = tile_of(n, wide)
            stream = residual_ref[:, cols].astype(jnp.float32)
            stream = stream + projected[:, cols] * norm * mixer_gain_ref[:, cols]
            stream = stream.astype(half)
            stream_ref[:, cols] = stream
            squares(stream.astype(jnp.float32))

        norm2 = inverse_root()

        @pl.loop(0, model // wide)
        def _(n):
            cols = tile_of(n, wide)
            normed = stream_ref[:, cols].astype(jnp.float32) * norm2 * channel_gain_ref[:, cols]
            normed_ref[:, cols] = normed.astype(half)

    def send_out(k):
        return remote(outgoing.at[k], arrived.at[k, 0, 0], a_send.at[0], a_recv.at[k], sp_at(k))

    def cross_out(k, j):
        return remote(arrived.at[k, 0, 0], arrived.at[k, 0, j], b_send.at[0], b_recv.at[k, j - 1], chip_at(j))

    def twin_out(k, j):
        return remote(arrived.at[k, 0, j], arrived.at[k, 1, j], c_send.at[0], c_recv.at[k], other)

    def pair_rows(k, j):
        return pl.ds(pl.multiple_of((k * groups + j) * capacity, capacity), capacity)

    def pair_out(k, j):
        return remote(arrived.at[k, 1, j], pool.at[pair_rows(k, j)], d_send.at[0], d_recv.at[k], other)

    def cross_back(k, j):
        return remote(own.at[k, j], cross_in.at[k, j - 1], e_send.at[0], e_recv.at[k, j - 1], chip_at(-j))

    def send_back(k):
        return remote(own.at[k, 0], returned.at[k], f_send.at[0], f_recv.at[0], sp_at(k))

    near = count // 2

    def gather(first):
        @pl.loop(0, model // wide)
        def _(n):
            cols = tile_of(n, wide)
            chosen = place_ref[first * capacity : (first + near) * capacity, :]
            block = jnp.dot(chosen, normed_ref[:, cols], preferred_element_type=jnp.float32)
            block = block.astype(half).reshape(near, capacity, wide)
            outgoing[first : first + near, :, cols] = block
            if first == 0:
                arrived[0, 0, 0, :, cols] = block[0]

    def forward(k):
        @pl.when(k > 0)
        def _():
            with scope("A_wait"):
                send_out(k).wait_recv()

        for j in range(1, groups):
            cross_out(k, j).start()
        twin_out(k, 0).start()

    with scope("gather"):
        gather(0)

        @pl.loop(1, near)
        def _(k):
            send_out(k).start()

        forward(0)
        gather(near)

        @pl.loop(near, count)
        def _(k):
            send_out(k).start()

    def forward_twin(k):
        for j in range(1, groups):
            with scope("Y_wait"):
                cross_out(k, j).wait_recv()
            twin_out(k, j).start()

    def complete(k):
        with scope("twin_wait"):
            wait_bytes(arrived.at[k, 1], c_recv.at[k])

    def pair_sum(k):
        held_rows = pl.ds(pl.multiple_of(k * groups * capacity, capacity), groups * capacity)
        with scope("pair_wait"):
            wait_bytes(pool.at[held_rows], d_recv.at[k])
        for j in range(groups):
            given = pool[pair_rows(k, j), :].astype(jnp.float32)
            own[k, j] = (own[k, j].astype(jnp.float32) + given).astype(half)
        for j in range(1, groups):
            cross_back(k, j).start()

    def total(k):
        value = own[k, 0].astype(jnp.float32)
        for j in range(1, groups):
            with scope("B_wait"):
                cross_back(k, j).wait_recv()
            value = value + cross_in[k, j - 1].astype(jnp.float32)
        value = value.astype(half)

        @pl.when(k > 0)
        def _():
            own[k, 0] = value
            send_back(k).start()

        @pl.when(k == 0)
        def _():
            returned[k] = value

    tile = math.gcd(units, 256)
    held = 2 * groups * capacity

    def expand(k):
        complete(k)

        with scope("ffn_up"):
            @pl.loop(0, units // tile)
            def _(n):
                cols = tile_of(n, tile)
                value = arrived[k].reshape(held, model)
                gate = jnp.dot(value, gate_w[:, cols], preferred_element_type=jnp.float32)
                up = jnp.dot(value, up_w[:, cols], preferred_element_type=jnp.float32)
                hidden[:, cols] = (gate / (1.0 + jnp.exp(-gate)) * up).astype(half)

    def contract(k):
        with scope("ffn_down"):
            @pl.loop(0, model // wide)
            def _(n):
                cols = tile_of(n, wide)
                part = jnp.dot(hidden[...], down_w[:, cols], preferred_element_type=jnp.float32)
                part = part.astype(half).reshape(2, groups, capacity, wide)
                own[k, :, :, cols] = part[0]
                arrived[k, 1, :, :, cols] = part[1]

        for j in range(groups):
            pair_out(k, j).start()

    for copy in expert_loads:
        copy.wait()

    kinds = (forward, forward_twin, expand, contract, pair_sum, total)
    inner, outer = ([kind * count + k for kind, k in plan(count, eight)] for eight in (INNER, OUTER))
    ends = (me < count // 4) | (me >= count - count // 4)

    @pl.loop(0, len(inner))
    def _(i):
        code = 0
        for n in range(len(inner)):
            value = inner[n] if inner[n] == outer[n] else jnp.where(ends, outer[n], inner[n])
            code = jnp.where(i == n, value, code)
        for kind, action in enumerate(kinds):

            @pl.when(code // count == kind)
            def _():
                action(code % count)

    square_ref[...] = jnp.zeros_like(square_ref)

    with scope("wait_back"):
        wait_bytes(returned.at[1:count], f_recv.at[0])

    with scope("combine"):
        @pl.loop(0, model // wide)
        def _(n):
            cols = tile_of(n, wide)
            back = returned[:, :, cols].reshape(slots, wide)
            piece = jnp.dot(high_ref[...], back, preferred_element_type=jnp.float32)
            piece = piece + jnp.dot(low_ref[...], back, preferred_element_type=jnp.float32)
            projected[:, cols] = piece
            squares(piece)

        norm3 = inverse_root()

        def out_copy(n):
            cols = tile_of(n, wide)
            return pltpu.make_async_copy(normed_ref.at[:, cols], out_hbm.at[:, cols], out_sem.at[0])

        @pl.loop(0, model // wide)
        def _(n):
            cols = tile_of(n, wide)
            value = stream_ref[:, cols].astype(jnp.float32)
            value = value + projected[:, cols] * norm3 * expert_gain_ref[:, cols]
            normed_ref[:, cols] = value.astype(half)
            out_copy(n).start()

    with scope("drain"):
        for h in range(heads):
            for i in range(3):
                wait_bytes(value_in.at[h, 1:count], in_send.at[h, i])
            wait_bytes(head_out.at[h, 1:count], head_send.at[h])
        wait_bytes(outgoing.at[1:count], a_send.at[0])
        if groups > 1:
            wait_bytes(cross_in, b_send.at[0])
            wait_bytes(cross_in, e_send.at[0])
        wait_bytes(own, c_send.at[0])
        wait_bytes(own, d_send.at[0])
        wait_bytes(returned.at[1:count], f_send.at[0])
        wait_bytes(normed_ref, out_sem.at[0])


def local(
    queries,
    key_rows,
    value_rows,
    lambdas,
    head_gain,
    out_weight,
    residual,
    mixer_gain,
    channel_gain,
    expert_gain,
    routes,
    route_logits,
    gate_weight,
    up_weight,
    down_weight,
):
    count, groups = lax.axis_size("sp"), lax.axis_size("dp") // 2
    heads = lambdas.shape[0]
    lanes = head_gain.shape[0]
    map_dim = lanes // 2
    _, tokens, model = residual.shape
    units = gate_weight.shape[2]
    capacity = -(-max(2, 3 * tokens // count) // 16) * 16
    slots = count * capacity
    inverse = 1.0 / np.float32(10000.0) ** (np.arange(0, map_dim, 2, dtype=np.float32) / np.float32(map_dim))
    angles = np.arange(count * tokens, dtype=np.float32)[:, None] * inverse.astype(np.float32)[None, :]
    cosine = np.cos(angles.astype(np.float64)).astype(np.float32)
    sine = np.sin(angles.astype(np.float64)).astype(np.float32)
    cos_table = jnp.asarray(np.concatenate([cosine] * 4, axis=1))
    sin_table = jnp.asarray(np.concatenate([-sine, sine] * 2, axis=1))
    vmem = pl.BlockSpec(memory_space=pltpu.VMEM)
    smem = pl.BlockSpec(memory_space=pltpu.SMEM)
    anywhere = pl.BlockSpec(memory_space=pl.ANY)
    half = jnp.bfloat16
    dma = pltpu.SemaphoreType.DMA
    rows = pltpu.VMEM((tokens, model), half)
    blocks = pltpu.VMEM((heads, count, tokens, lanes), half)
    table = pltpu.VMEM((tokens, lanes), jnp.float32)
    pool_rows = max(out_weight.shape[0], slots * groups)
    wide = math.gcd(model, 512)
    updated = pl.pallas_call(
        functools.partial(layer_kernel, count, groups),
        out_shape=jax.ShapeDtypeStruct((tokens, model), half),
        in_specs=[anywhere] * 5 + [smem, vmem, anywhere] + [vmem] * 5 + [anywhere] * 4,
        out_specs=anywhere,
        scratch_shapes=[
            rows,
            rows,
            rows,
            table,
            table,
            rows,
            blocks,
            blocks,
            blocks,
            blocks,
            blocks,
            blocks,
            pltpu.VMEM((heads, tokens, count * lanes), half),
            pltpu.VMEM((tokens, model), jnp.float32),
            pltpu.VMEM((tokens, 128), jnp.float32),
            rows,
            rows,
            pltpu.VMEM((slots, tokens), half),
            pltpu.VMEM((tokens, slots), half),
            pltpu.VMEM((tokens, slots), half),
            pltpu.VMEM((pool_rows, model), half),
            pltpu.VMEM((count, capacity, model), half),
            pltpu.VMEM((count, 2, groups, capacity, model), half),
            pltpu.VMEM((count, groups, capacity, model), half),
            pltpu.VMEM((count, max(1, groups - 1), capacity, model), half),
            pltpu.VMEM((count, capacity, model), half),
            pltpu.VMEM((2 * groups * capacity, units), half),
            pltpu.VMEM((model, units), half),
            pltpu.VMEM((model, units), half),
            pltpu.VMEM((units, model), half),
            dma((6,)),
            dma((heads,)),
            dma((3,)),
            dma((1,)),
            dma((heads, 3)),
            dma((heads, 2)),
            dma((heads, count // WIDTH)),
            dma((heads,)),
            dma((heads, count)),
            dma((1,)),
            dma((count,)),
            dma((1,)),
            dma((count, max(1, groups - 1))),
            dma((1,)),
            dma((count,)),
            dma((1,)),
            dma((count,)),
            dma((1,)),
            dma((count, max(1, groups - 1))),
            dma((1,)),
            dma((1,)),
        ],
        compiler_params=pltpu.CompilerParams(
            collective_id=1, has_side_effects=True, vmem_limit_bytes=67043328
        ),
        name="layer",
    )(
        queries[0],
        key_rows[0],
        value_rows[0],
        cos_table,
        sin_table,
        lambdas,
        head_gain[None, :],
        residual[0],
        mixer_gain[None, :],
        channel_gain[None, :],
        expert_gain[None, :],
        routes[0].T,
        route_logits[0].T,
        out_weight,
        gate_weight[0],
        up_weight[0],
        down_weight[0],
    )
    return updated[None]


def solution(mesh):
    placed = (
        P("dp", "sp", None),
        P("dp", "sp", None),
        P("dp", "sp", None),
        P("sp"),
        P(),
        P(),
        P("dp", "sp", None),
        P(),
        P(),
        P(),
        P("dp", "sp", None),
        P("dp", "sp", None),
        P("sp", None, "dp"),
        P("sp", None, "dp"),
        P("sp", "dp", None),
    )
    return jax.shard_map(
        local, mesh=mesh, in_specs=placed, out_specs=P("dp", "sp", None), check_vma=False
    )
```

```python
import contextlib
import functools
import math

import jax
import jax.numpy as jnp
import numpy as np
from jax import lax
from jax.experimental import pallas as pl
from jax.experimental.pallas import tpu as pltpu
from jax.sharding import PartitionSpec as P


MESH = pl.DeviceIdType.MESH
WIDTH = 2
TRACE = False


def scope(name):
    return jax.named_scope(name) if TRACE else contextlib.nullcontext()


KINDS = "AYUDPT"
INNER = (
    "A1", "Y0", "U0", "D0", "A2", "Y1", "U1", "A4", "D1", "A3", "Y2", "U2", "Y4", "D2", "A5", "U4",
    "D4", "Y3", "P4", "Y5", "A6", "U5", "A7", "D5", "T4", "U3", "P5", "P1", "D3", "Y6", "U6", "D6",
    "T5", "P6", "P2", "Y7", "U7", "T6", "D7", "P7", "P3", "P0", "T1", "T2", "T7", "T3", "T0",
)
OUTER = (
    "A1", "Y0", "U0", "D0", "A2", "Y1", "U1", "A4", "D1", "A3", "Y2", "U2", "Y4", "P1", "D2", "U4",
    "A5", "D4", "Y3", "P4", "Y5", "U3", "A6", "D3", "U5", "T4", "D5", "A7", "P5", "Y6", "U6", "D6",
    "T5", "P6", "P2", "Y7", "U7", "D7", "T6", "P7", "P3", "P0", "T1", "T7", "T2", "T3", "T0",
)


def plan(count, eight):
    if count == 8:
        return [(KINDS.index(step[0]), int(step[1:])) for step in eight]
    steps = []
    for n in range(count + 3):
        if 0 < n < count:
            steps.append((KINDS.index("A"), n))
        if 2 <= n < count + 2:
            steps.append((KINDS.index("P"), n - 2))
        if n >= 3:
            steps.append((KINDS.index("T"), n - 3))
        if 1 <= n <= count:
            steps += [(KINDS.index(kind), n - 1) for kind in "YUD"]
    return steps


def layer_kernel(
    count,
    groups,
    query_hbm,
    key_hbm,
    value_hbm,
    cos_hbm,
    sin_hbm,
    lambda_ref,
    head_gain_ref,
    residual_hbm,
    mixer_gain_ref,
    channel_gain_ref,
    expert_gain_ref,
    routes_ref,
    logits_ref,
    weight_hbm,
    gate_hbm,
    up_hbm,
    down_hbm,
    out_hbm,
    query_ref,
    key_ref,
    value_ref,
    cos_ref,
    sin_ref,
    residual_ref,
    query_out,
    key_out,
    query_in,
    key_in,
    value_in,
    head_out,
    token_rows,
    projected,
    square_ref,
    stream_ref,
    normed_ref,
    place_ref,
    high_ref,
    low_ref,
    pool,
    outgoing,
    arrived,
    own,
    cross_in,
    returned,
    hidden,
    gate_w,
    up_w,
    down_w,
    in_sem,
    weight_sem,
    expert_sem,
    out_sem,
    in_send,
    kv_recv,
    query_recv,
    head_send,
    head_recv,
    a_send,
    a_recv,
    b_send,
    b_recv,
    c_send,
    c_recv,
    d_send,
    d_recv,
    e_send,
    e_recv,
    f_send,
    f_recv,
):
    me = lax.axis_index("sp")
    dp = lax.axis_index("dp")
    chip, core = dp // 2, dp % 2
    tokens, model = query_ref.shape
    lanes = head_gain_ref.shape[1]
    heads = lambda_ref.shape[0]
    map_dim = lanes // 2
    scale = map_dim ** (-0.5)
    capacity = outgoing.shape[1]
    units = gate_w.shape[1]
    wide = math.gcd(model, 1024)
    half = jnp.bfloat16

    def peer(k):
        total, bit = 0, 1
        while bit < count:
            a, b = (me // bit) % 2, (k // bit) % 2
            total = total + bit * (a + b - 2 * a * b)
            bit *= 2
        return total

    other = {"sp": me, "dp": chip * 2 + (1 - core)}

    def chip_at(step):
        return {"sp": me, "dp": ((chip + step + groups) % groups) * 2 + core}

    def sp_at(k):
        return {"sp": peer(k), "dp": dp}

    def columns(owner, h):
        return pl.ds(pl.multiple_of((owner * heads + h) * lanes, lanes), lanes)

    def tile_of(n, size):
        return pl.ds(pl.multiple_of(n * size, size), size)

    def remote(src, dst, send, recv, device):
        return pltpu.make_async_remote_copy(
            src_ref=src, dst_ref=dst, send_sem=send, recv_sem=recv, device_id=device, device_id_type=MESH
        )

    rows_here = pl.ds(pl.multiple_of(me * tokens, tokens), tokens)
    inputs = [
        pltpu.make_async_copy(src, dst, in_sem.at[i])
        for i, (src, dst) in enumerate(
            (
                (value_hbm, value_ref),
                (key_hbm, key_ref),
                (cos_hbm.at[rows_here], cos_ref),
                (sin_hbm.at[rows_here], sin_ref),
                (query_hbm, query_ref),
                (residual_hbm, residual_ref),
            )
        )
    ]
    for copy in inputs:
        copy.start()

    def weight_load(h, o):
        return pltpu.make_async_copy(
            weight_hbm.at[columns(o, h)],
            pool.at[pl.ds(pl.multiple_of((h * count + o) * lanes, lanes), lanes)],
            weight_sem.at[h],
        )

    expert_loads = [
        pltpu.make_async_copy(src, dst, expert_sem.at[i])
        for i, (src, dst) in enumerate(((gate_hbm, gate_w), (up_hbm, up_w), (down_hbm, down_w)))
    ]

    barrier = pltpu.get_barrier_semaphore()
    peers = [sp_at(k) for k in range(1, count)] + [chip_at(j) for j in range(1, groups)] + [other]
    for device in peers:
        pl.semaphore_signal(barrier, inc=1, device_id=device, device_id_type=MESH)

    def wait_bytes(ref, sem):
        pltpu.make_async_copy(ref, ref, sem).wait()

    def inward(h, k, i):
        sources = (value_ref.at[:, columns(peer(k), h)], query_out.at[h, k], key_out.at[h, k])
        targets = (value_in.at[h, k], query_in.at[h, k], key_in.at[h, k])
        landed = (kv_recv.at[h, 0], query_recv.at[h, k // WIDTH], kv_recv.at[h, 1])
        return remote(sources[i], targets[i], in_send.at[h, i], landed[i], sp_at(k))

    def outward(h, k):
        return remote(
            head_out.at[h, k],
            token_rows.at[h, :, tile_of(me, lanes)],
            head_send.at[h],
            head_recv.at[h, k],
            sp_at(k),
        )

    first_half = lax.broadcasted_iota(jnp.int32, (tokens, lanes), 1) % map_dim < map_dim // 2

    def turned(ref, cols):
        x = ref[:, cols].astype(jnp.float32)
        ahead = pltpu.roll(x, lanes - map_dim // 2, 1)
        behind = pltpu.roll(x, map_dim // 2, 1)
        return x * cos_ref[...] + jnp.where(first_half, ahead, behind) * sin_ref[...]

    def turned_query(cols):
        return (turned(query_ref, cols) * scale).astype(half)

    def turned_key(cols):
        return turned(key_ref, cols).astype(half)

    with scope("barrier"):
        inputs[0].wait()
        pl.semaphore_wait(barrier, len(peers))

    with scope("prepare"):
        for h in range(heads):

            @pl.loop(1, count)
            def _(k):
                inward(h, k, 0).start()

            if h == 0:
                for copy in inputs[1:4]:
                    copy.wait()

            @pl.loop(1, count)
            def _(k):
                key_out[h, k] = turned_key(columns(peer(k), h))

            @pl.loop(1, count)
            def _(k):
                inward(h, k, 2).start()

            if h == 0:
                inputs[4].wait()

            @pl.loop(1, count)
            def _(k):
                query_out[h, k] = turned_query(columns(peer(k), h))

            @pl.loop(1, count)
            def _(k):
                inward(h, count - k, 1).start()

        for h in range(heads):
            query_in[h, 0] = turned_query(columns(me, h))
            key_in[h, 0] = turned_key(columns(me, h))
            value_in[h, 0] = value_ref[:, columns(me, h)]

        for h in range(heads):

            @pl.loop(0, count)
            def _(o):
                weight_load(h, o).start()

        for copy in expert_loads:
            copy.start()

    with scope("routing"):
        top = routes_ref.shape[0]
        slots = count * capacity
        ranks = max(16, count)
        experts = lax.broadcasted_iota(jnp.int32, (ranks, tokens), 0)
        places = lax.broadcasted_iota(jnp.int32, (slots, tokens), 0)
        upper = lax.broadcasted_iota(jnp.int32, (tokens, tokens), 0)
        upper = (upper <= lax.broadcasted_iota(jnp.int32, (tokens, tokens), 1)).astype(half)
        logits = logits_ref[...]
        odds = jnp.exp(logits - jnp.max(logits, axis=0, keepdims=True))
        shares = odds / jnp.sum(odds, axis=0, keepdims=True)
        used = jnp.zeros((ranks, 1), jnp.float32)
        mix = jnp.zeros((slots, tokens), jnp.float32)
        place = jnp.zeros((slots, tokens), jnp.float32)
        for i in range(top):
            ranked = jnp.bitwise_xor(routes_ref[i : i + 1, :], me)
            named = (experts == ranked).astype(jnp.float32)
            running = jnp.dot(named.astype(half), upper, preferred_element_type=jnp.float32)
            slot = jnp.sum(named * (running + used), axis=0, keepdims=True).astype(jnp.int32) - 1
            used = used + jnp.sum(named, axis=1, keepdims=True)
            hit = places == ranked * capacity + slot
            mix = mix + jnp.where(hit, shares[i : i + 1, :], 0.0)
            place = place + jnp.where(hit, 1.0, 0.0)
        place_ref[...] = place.astype(half)
        mix = mix.T
        high = mix.astype(half)
        high_ref[...] = high
        low_ref[...] = (mix - high.astype(jnp.float32)).astype(half)

    rows = WIDTH * tokens
    length = count * tokens
    in_first = lax.broadcasted_iota(jnp.int32, (rows, lanes), 1) < map_dim

    def part_of(total):
        return jnp.exp(total - jnp.max(total, axis=-1, keepdims=True))

    for h in range(heads):

        with scope("wait_kv"):
            wait_bytes(value_in.at[h, 1:count], kv_recv.at[h, 0])
            wait_bytes(key_in.at[h, 1:count], kv_recv.at[h, 1])

        @pl.loop(0, count // WIDTH)
        def _(step):
            b = count // WIDTH - 1 - step
            with scope("wait_q"):
                @pl.when(b > 0)
                def _():
                    wait_bytes(query_in.at[h, pl.ds(b * WIDTH, WIDTH)], query_recv.at[h, b])

                @pl.when(b == 0)
                def _():
                    wait_bytes(query_in.at[h, 1:WIDTH], query_recv.at[h, b])

            with scope("attend"):
                query = query_in[h, pl.ds(b * WIDTH, WIDTH)].reshape(rows, lanes).astype(jnp.float32)
                both = jnp.concatenate(
                    [jnp.where(in_first, query, 0.0), jnp.where(in_first, 0.0, query)], axis=0
                ).astype(half)
                keys = key_in[h].reshape(length, lanes)
                scores = lax.dot_general(
                    both, keys, (((1,), (1,)), ((), ())), preferred_element_type=jnp.float32
                )
                one, two = part_of(scores[:rows]), part_of(scores[rows:])
                one_scale = 1.0 / jnp.sum(one, axis=-1, keepdims=True)
                two_scale = lambda_ref[h] / jnp.sum(two, axis=-1, keepdims=True)
                mixing = (one * one_scale - two * two_scale).astype(half)
                mixed = jnp.dot(
                    mixing, value_in[h].reshape(length, lanes), preferred_element_type=jnp.float32
                )
                norm = lax.rsqrt(jnp.mean(mixed * mixed, axis=-1, keepdims=True) + 1e-05)
                result = (mixed * norm * head_gain_ref[...]).astype(half)
                head_out[h, pl.ds(b * WIDTH, WIDTH)] = result.reshape(WIDTH, tokens, lanes)
            for i in range(WIDTH):
                k = b * WIDTH + i

                @pl.when(k > 0)
                def _():
                    outward(h, k).start()

    for h in range(heads):
        token_rows[h, :, tile_of(me, lanes)] = head_out[h, 0]

    depth = count * lanes
    square_ref[...] = jnp.zeros_like(square_ref)

    def squares(value):
        value = value * value
        total = value[:, :128]
        for i in range(1, wide // 128):
            total = total + value[:, i * 128 : (i + 1) * 128]
        square_ref[...] += total

    def inverse_root():
        total = jnp.sum(square_ref[...], axis=-1, keepdims=True)
        return lax.rsqrt(total / model + 1e-06)

    for h in range(heads):

        wait_bytes(pool.at[h * depth : (h + 1) * depth], weight_sem.at[h])

        with scope("wait_heads"):
            @pl.loop(1, count)
            def _(k):
                outward(h, k).wait_recv()

        with scope("project"):
            @pl.loop(0, model // wide)
            def _(n):
                cols = tile_of(n, wide)
                value = jnp.dot(
                    token_rows[h], pool[h * depth : (h + 1) * depth, cols], preferred_element_type=jnp.float32
                )
                if h > 0:
                    value = value + projected[:, cols]
                projected[:, cols] = value
                if h == heads - 1:
                    squares(value)

    with scope("norms"):
        norm = inverse_root()
        square_ref[...] = jnp.zeros_like(square_ref)
        inputs[5].wait()

        @pl.loop(0, model // wide)
        def _(n):
            cols = tile_of(n, wide)
            stream = residual_ref[:, cols].astype(jnp.float32)
            stream = stream + projected[:, cols] * norm * mixer_gain_ref[:, cols]
            stream = stream.astype(half)
            stream_ref[:, cols] = stream
            squares(stream.astype(jnp.float32))

        norm2 = inverse_root()

        @pl.loop(0, model // wide)
        def _(n):
            cols = tile_of(n, wide)
            normed = stream_ref[:, cols].astype(jnp.float32) * norm2 * channel_gain_ref[:, cols]
            normed_ref[:, cols] = normed.astype(half)

    def send_out(k):
        return remote(outgoing.at[k], arrived.at[k, 0, 0], a_send.at[0], a_recv.at[k], sp_at(k))

    def cross_out(k, j):
        return remote(arrived.at[k, 0, 0], arrived.at[k, 0, j], b_send.at[0], b_recv.at[k, j - 1], chip_at(j))

    def twin_out(k, j):
        return remote(arrived.at[k, 0, j], arrived.at[k, 1, j], c_send.at[0], c_recv.at[k], other)

    def pair_rows(k, j):
        return pl.ds(pl.multiple_of((k * groups + j) * capacity, capacity), capacity)

    def pair_out(k, j):
        return remote(arrived.at[k, 1, j], pool.at[pair_rows(k, j)], d_send.at[0], d_recv.at[k], other)

    def cross_back(k, j):
        return remote(own.at[k, j], cross_in.at[k, j - 1], e_send.at[0], e_recv.at[k, j - 1], chip_at(-j))

    def send_back(k):
        return remote(own.at[k, 0], returned.at[k], f_send.at[0], f_recv.at[0], sp_at(k))

    near = count // 2

    def gather(first):
        @pl.loop(0, model // wide)
        def _(n):
            cols = tile_of(n, wide)
            chosen = place_ref[first * capacity : (first + near) * capacity, :]
            block = jnp.dot(chosen, normed_ref[:, cols], preferred_element_type=jnp.float32)
            block = block.astype(half).reshape(near, capacity, wide)
            outgoing[first : first + near, :, cols] = block
            if first == 0:
                arrived[0, 0, 0, :, cols] = block[0]

    def forward(k):
        @pl.when(k > 0)
        def _():
            with scope("A_wait"):
                send_out(k).wait_recv()

        for j in range(1, groups):
            cross_out(k, j).start()
        twin_out(k, 0).start()

    with scope("gather"):
        gather(0)

        @pl.loop(1, near)
        def _(k):
            send_out(k).start()

        forward(0)
        gather(near)

        @pl.loop(near, count)
        def _(k):
            send_out(k).start()

    def forward_twin(k):
        for j in range(1, groups):
            with scope("Y_wait"):
                cross_out(k, j).wait_recv()
            twin_out(k, j).start()

    def complete(k):
        with scope("twin_wait"):
            wait_bytes(arrived.at[k, 1], c_recv.at[k])

    def pair_sum(k):
        held_rows = pl.ds(pl.multiple_of(k * groups * capacity, capacity), groups * capacity)
        with scope("pair_wait"):
            wait_bytes(pool.at[held_rows], d_recv.at[k])
        for j in range(groups):
            given = pool[pair_rows(k, j), :].astype(jnp.float32)
            own[k, j] = (own[k, j].astype(jnp.float32) + given).astype(half)
        for j in range(1, groups):
            cross_back(k, j).start()

    def total(k):
        value = own[k, 0].astype(jnp.float32)
        for j in range(1, groups):
            with scope("B_wait"):
                cross_back(k, j).wait_recv()
            value = value + cross_in[k, j - 1].astype(jnp.float32)
        value = value.astype(half)

        @pl.when(k > 0)
        def _():
            own[k, 0] = value
            send_back(k).start()

        @pl.when(k == 0)
        def _():
            returned[k] = value

    tile = math.gcd(units, 512)
    held = 2 * groups * capacity

    def expand(k):
        complete(k)

        with scope("ffn_up"):
            @pl.loop(0, units // tile)
            def _(n):
                cols = tile_of(n, tile)
                value = arrived[k].reshape(held, model)
                gate = jnp.dot(value, gate_w[:, cols], preferred_element_type=jnp.float32)
                up = jnp.dot(value, up_w[:, cols], preferred_element_type=jnp.float32)
                hidden[:, cols] = (gate / (1.0 + jnp.exp(-gate)) * up).astype(half)

    broad = math.gcd(model, 2048)

    def contract(k):
        with scope("ffn_down"):
            @pl.loop(0, model // broad)
            def _(n):
                cols = tile_of(n, broad)
                part = jnp.dot(hidden[...], down_w[:, cols], preferred_element_type=jnp.float32)
                part = part.astype(half).reshape(2, groups, capacity, broad)
                own[k, :, :, cols] = part[0]
                arrived[k, 1, :, :, cols] = part[1]

        for j in range(groups):
            pair_out(k, j).start()

    for copy in expert_loads:
        copy.wait()

    kinds = (forward, forward_twin, expand, contract, pair_sum, total)
    inner, outer = ([kind * count + k for kind, k in plan(count, eight)] for eight in (INNER, OUTER))
    ends = (me < count // 4) | (me >= count - count // 4)

    @pl.loop(0, len(inner))
    def _(i):
        code = 0
        for n in range(len(inner)):
            value = inner[n] if inner[n] == outer[n] else jnp.where(ends, outer[n], inner[n])
            code = jnp.where(i == n, value, code)
        for kind, action in enumerate(kinds):

            @pl.when(code // count == kind)
            def _():
                action(code % count)

    square_ref[...] = jnp.zeros_like(square_ref)

    with scope("wait_back"):
        wait_bytes(returned.at[1:count], f_recv.at[0])

    with scope("combine"):
        @pl.loop(0, model // wide)
        def _(n):
            cols = tile_of(n, wide)
            back = returned[:, :, cols].reshape(slots, wide)
            piece = jnp.dot(high_ref[...], back, preferred_element_type=jnp.float32)
            piece = piece + jnp.dot(low_ref[...], back, preferred_element_type=jnp.float32)
            projected[:, cols] = piece
            squares(piece)

        norm3 = inverse_root()

        def out_copy(n):
            cols = tile_of(n, wide)
            return pltpu.make_async_copy(normed_ref.at[:, cols], out_hbm.at[:, cols], out_sem.at[0])

        @pl.loop(0, model // wide)
        def _(n):
            cols = tile_of(n, wide)
            value = stream_ref[:, cols].astype(jnp.float32)
            value = value + projected[:, cols] * norm3 * expert_gain_ref[:, cols]
            normed_ref[:, cols] = value.astype(half)
            out_copy(n).start()

    with scope("drain"):
        for h in range(heads):
            for i in range(3):
                wait_bytes(value_in.at[h, 1:count], in_send.at[h, i])
            wait_bytes(head_out.at[h, 1:count], head_send.at[h])
        wait_bytes(outgoing.at[1:count], a_send.at[0])
        if groups > 1:
            wait_bytes(cross_in, b_send.at[0])
            wait_bytes(cross_in, e_send.at[0])
        wait_bytes(own, c_send.at[0])
        wait_bytes(own, d_send.at[0])
        wait_bytes(returned.at[1:count], f_send.at[0])
        wait_bytes(normed_ref, out_sem.at[0])


def local(
    queries,
    key_rows,
    value_rows,
    lambdas,
    head_gain,
    out_weight,
    residual,
    mixer_gain,
    channel_gain,
    expert_gain,
    routes,
    route_logits,
    gate_weight,
    up_weight,
    down_weight,
):
    count, groups = lax.axis_size("sp"), lax.axis_size("dp") // 2
    heads = lambdas.shape[0]
    lanes = head_gain.shape[0]
    map_dim = lanes // 2
    _, tokens, model = residual.shape
    units = gate_weight.shape[2]
    capacity = -(-max(2, 3 * tokens // count) // 16) * 16
    slots = count * capacity
    inverse = 1.0 / np.float32(10000.0) ** (np.arange(0, map_dim, 2, dtype=np.float32) / np.float32(map_dim))
    angles = np.arange(count * tokens, dtype=np.float32)[:, None] * inverse.astype(np.float32)[None, :]
    cosine = np.cos(angles.astype(np.float64)).astype(np.float32)
    sine = np.sin(angles.astype(np.float64)).astype(np.float32)
    cos_table = jnp.asarray(np.concatenate([cosine] * 4, axis=1))
    sin_table = jnp.asarray(np.concatenate([-sine, sine] * 2, axis=1))
    vmem = pl.BlockSpec(memory_space=pltpu.VMEM)
    smem = pl.BlockSpec(memory_space=pltpu.SMEM)
    anywhere = pl.BlockSpec(memory_space=pl.ANY)
    half = jnp.bfloat16
    dma = pltpu.SemaphoreType.DMA
    rows = pltpu.VMEM((tokens, model), half)
    blocks = pltpu.VMEM((heads, count, tokens, lanes), half)
    table = pltpu.VMEM((tokens, lanes), jnp.float32)
    pool_rows = max(out_weight.shape[0], slots * groups)
    wide = math.gcd(model, 1024)
    updated = pl.pallas_call(
        functools.partial(layer_kernel, count, groups),
        out_shape=jax.ShapeDtypeStruct((tokens, model), half),
        in_specs=[anywhere] * 5 + [smem, vmem, anywhere] + [vmem] * 5 + [anywhere] * 4,
        out_specs=anywhere,
        scratch_shapes=[
            rows,
            rows,
            rows,
            table,
            table,
            rows,
            blocks,
            blocks,
            blocks,
            blocks,
            blocks,
            blocks,
            pltpu.VMEM((heads, tokens, count * lanes), half),
            pltpu.VMEM((tokens, model), jnp.float32),
            pltpu.VMEM((tokens, 128), jnp.float32),
            rows,
            rows,
            pltpu.VMEM((slots, tokens), half),
            pltpu.VMEM((tokens, slots), half),
            pltpu.VMEM((tokens, slots), half),
            pltpu.VMEM((pool_rows, model), half),
            pltpu.VMEM((count, capacity, model), half),
            pltpu.VMEM((count, 2, groups, capacity, model), half),
            pltpu.VMEM((count, groups, capacity, model), half),
            pltpu.VMEM((count, max(1, groups - 1), capacity, model), half),
            pltpu.VMEM((count, capacity, model), half),
            pltpu.VMEM((2 * groups * capacity, units), half),
            pltpu.VMEM((model, units), half),
            pltpu.VMEM((model, units), half),
            pltpu.VMEM((units, model), half),
            dma((6,)),
            dma((heads,)),
            dma((3,)),
            dma((1,)),
            dma((heads, 3)),
            dma((heads, 2)),
            dma((heads, count // WIDTH)),
            dma((heads,)),
            dma((heads, count)),
            dma((1,)),
            dma((count,)),
            dma((1,)),
            dma((count, max(1, groups - 1))),
            dma((1,)),
            dma((count,)),
            dma((1,)),
            dma((count,)),
            dma((1,)),
            dma((count, max(1, groups - 1))),
            dma((1,)),
            dma((1,)),
        ],
        compiler_params=pltpu.CompilerParams(
            collective_id=1, has_side_effects=True, vmem_limit_bytes=67043328
        ),
        name="layer",
    )(
        queries[0],
        key_rows[0],
        value_rows[0],
        cos_table,
        sin_table,
        lambdas,
        head_gain[None, :],
        residual[0],
        mixer_gain[None, :],
        channel_gain[None, :],
        expert_gain[None, :],
        routes[0].T,
        route_logits[0].T,
        out_weight,
        gate_weight[0],
        up_weight[0],
        down_weight[0],
    )
    return updated[None]


def solution(mesh):
    placed = (
        P("dp", "sp", None),
        P("dp", "sp", None),
        P("dp", "sp", None),
        P("sp"),
        P(),
        P(),
        P("dp", "sp", None),
        P(),
        P(),
        P(),
        P("dp", "sp", None),
        P("dp", "sp", None),
        P("sp", None, "dp"),
        P("sp", None, "dp"),
        P("sp", "dp", None),
    )
    return jax.shard_map(
        local, mesh=mesh, in_specs=placed, out_specs=P("dp", "sp", None), check_vma=False
    )
```
